768 devices in a mesh: ep: 24 (over z, core), tp: 32 (over y, x).
Axes of the slice: x: 4, y: 8, z: 12, core: 2. Of those that a mesh axis runs over, the one named last changes fastest.
Arguments:
- hidden_in: bfloat16 [288, 2048], P('ep', 'tp'), may hold values from -12 to 12
- state: float32 [288, 32, 128, 128], P('ep', 'tp'), may hold values from -3 to 3
- lower_bound: float32 [32, 128], P('tp'), may hold values from 0.05 to 0.95
- w_forget: bfloat16 [2048, 4096], P(None, 'tp'), may hold values from -0.125 to 0.125
- w_input: bfloat16 [2048, 4096], P(None, 'tp'), may hold values from -0.125 to 0.125
- w_query: bfloat16 [2048, 4096], P(None, 'tp'), may hold values from -0.125 to 0.125
- w_outgate: bfloat16 [2048, 4096], P(None, 'tp'), may hold values from -0.125 to 0.125
- head_gain: float32 [128], replicated, may hold values from 0.1 to 1.9
- w_out: bfloat16 [4096, 2048], P('tp'), may hold values from -0.1875 to 0.1875
- ln1_gain: float32 [2048], replicated, may hold values from 0.1 to 8
- ln1_bias: float32 [2048], replicated, may hold values from -1.5 to 1.5
- routes: int32 [288, 4], P('ep'), may hold values from 0 to 47, all different within a row; in each aligned block of 12 rows (0 to 11, 12 to 23, ...) at most 2 rows name the same one
- route_weights: float32 [288, 4], P('ep'), may hold values from 0.2 to 1.5
- exp_gate: bfloat16 [48, 2048, 4096], P('ep', None, 'tp'), may hold values from -0.125 to 0.125
- exp_up: bfloat16 [48, 2048, 4096], P('ep', None, 'tp'), may hold values from -0.125 to 0.125
- exp_down: bfloat16 [48, 4096, 2048], P('ep', 'tp'), may hold values from -0.1875 to 0.1875
- sh_gate: bfloat16 [2048, 512], P(None, 'tp'), may hold values from -0.125 to 0.125
- sh_up: bfloat16 [2048, 512], P(None, 'tp'), may hold values from -0.125 to 0.125
- sh_down: bfloat16 [512, 2048], P('tp'), may hold values from -0.25 to 0.25
- ln2_gain: float32 [2048], replicated, may hold values from 0.1 to 1.9
- ln2_bias: float32 [2048], replicated, may hold values from -1.5 to 1.5
Outputs:
- mixed_out: bfloat16 [288, 2048], P('ep', 'tp')
- new_state: float32 [288, 32, 128, 128], P('ep', 'tp')
The draws below stay inside these ranges and needn't reach their ends.
Inputs may be any that keep to these rules, and one draw needn't show every extreme that they name: `routes`: each row names 4 different experts; among the rows of one index of ep (12 rows) no expert is named more than 2 times, a bound that some block reaches.
All inputs are finite; a program needn't handle non-finite values.
Results may differ from the reference program's by a relative error of at most 0.023.
Values may be sent and summed in bfloat16 or wider, within the bound.
A program may use at most 64 MiB of HBM per device.

```python
import math
import jax
import jax.numpy as jnp
import numpy as np
from jax import lax

D = 2048
HEAD = 128
HEADS = 32
HD = 4096
EFF = 4096
SFF = 512
TOPK = 4
EXPERTS = 48
SEQ_DEV = 12
BATCH = 288
CAP = 2
N_EP = 24
N_TP = 32


def draw_hidden_in(key, part):
    first_key = jax.random.fold_in(jax.random.fold_in(key, 11), 0)
    ramp = jnp.exp(jnp.log(3.0) * jnp.arange(D, dtype=jnp.float32) / D)
    values = jnp.clip(jax.random.normal(first_key, (BATCH, D), jnp.float32), -4.0, 4.0) * ramp
    return values.astype(jnp.bfloat16)


def draw_ln1_gain(key, part):
    noise_key = jax.random.fold_in(key, 23)
    noise = jax.random.uniform(noise_key, (D,), jnp.float32, -1.0, 1.0)
    ramp = jnp.exp(jnp.log(3.0) * jnp.arange(D, dtype=jnp.float32) / D)
    return ((1.0 + 0.18 * noise) * ramp).astype(jnp.float32)


def strengthened(array, key, source, target, blocks, factor):
    owner, partner = [(jnp.arange(array.shape[axis_at]) // (array.shape[axis_at] // blocks)).reshape([-1 if axis == axis_at else 1 for axis in range(array.ndim)]) for axis_at in (source, target)]
    chosen = jax.random.permutation(key, blocks)[partner]
    strong = (owner == chosen) | (owner == (partner + blocks // 2) % blocks)
    return jnp.where(strong, factor * array, array)


def steps_of(key, shape, shards, low, high):
    level = 1.0
    for dim, blocks in shards:
        steps = jax.random.uniform(jax.random.fold_in(jax.random.fold_in(key, 6), dim), (blocks,), jnp.float32, low / len(shards), high / len(shards))
        level = level * jnp.repeat(jnp.exp(steps), shape[dim] // blocks).reshape((-1,) + (1,) * (len(shape) - 1 - dim))
    return level


def routed_block(own_key, own, number, rows, count, top, limit, skew):
    order = jax.random.permutation(own_key, count)
    heavy_load, ordinary = shares(count, rows * top, limit, skew, True), shares(count, rows * top, limit, skew, False)
    places = jnp.arange(count)

    def named(tallies, offset_by):
        used = int((tallies > 0).sum())
        fixed = max(1, used // 4)
        passed = fixed + (places - fixed + offset_by * (used - fixed)) % max(1, count - fixed)
        return jnp.zeros((count,), jnp.int32).at[order[jnp.where(places < fixed, places, passed)]].set(jnp.asarray(tallies, jnp.int32))

    tallies = jnp.where(number % 4 == 0, named(heavy_load, number // 4), named(ordinary, number - number // 4 - 1))
    mixed = jax.random.permutation(jax.random.fold_in(own, 3), count)
    donor, sink = mixed[0:count // 2 * 2:2], mixed[1:count // 2 * 2:2]
    slack = jnp.minimum(tallies[donor] - 1, limit - tallies[sink]) // 2
    slack = jnp.where((donor == order[0]) | (sink == order[0]) | (tallies[sink] == 0), 0, jnp.maximum(slack, 0))
    passed = jax.random.randint(jax.random.fold_in(own, 4), (count // 2,), 0, 1 << 20) % (slack + 1)
    tallies = tallies.at[donor].add(-passed).at[sink].add(passed)
    items = jnp.searchsorted(jnp.cumsum(tallies), jnp.arange(rows * top), side="right").astype(jnp.int32)
    table = items.reshape(top, rows).T
    table = table[jax.random.permutation(jax.random.fold_in(own, 1), rows)]
    offset_by = jax.random.randint(jax.random.fold_in(own, 2), (rows, 1), 0, top)
    return jnp.take_along_axis(table, (jnp.arange(top)[None, :] + offset_by) % top, axis=1)


def shares(number_of, total, limit, slope, full):
    weights = [(1 << 20) // math.isqrt(rank ** slope) + 1 for rank in range(1, number_of + 1)]
    largest = limit if full else min(limit, max(-(-total // number_of), total * weights[0] // sum(weights)))
    least = 1 if total - largest >= number_of - 1 else 0
    given, spare = [largest] + [least] * (number_of - 1), total - largest - least * (number_of - 1)
    while spare > 0:
        movable = [i for i in range(1, number_of) if given[i] < largest] or [i for i in range(1, number_of) if given[i] < limit]
        pool, left = sum([weights[i] for i in movable]), spare
        for i in movable:
            more = min(limit - given[i], max(1, left * weights[i] // pool), spare)
            given[i] = given[i] + more
            spare = spare - more
    return np.array(given)


def scatter_about(rng, dims, scale, most, pieces=(), kind=jnp.bfloat16):
    entries = scale * jax.random.normal(rng, dims, jnp.float32)
    if pieces:
        entries = entries * steps_of(rng, dims, pieces, -0.22, 0.18)
    return jnp.clip(entries, -most, most).astype(kind)


def bell_draw_with(stream_key, dims, deviation, limit, cuts, heavy, kind=jnp.bfloat16):
    values = deviation * jax.random.normal(stream_key, dims, jnp.float32)
    if cuts:
        values = values * steps_of(stream_key, dims, cuts, -0.22, 0.18)
    return jnp.clip(strengthened(values, jax.random.fold_in(stream_key, 3), *heavy), -limit, limit).astype(kind)


def setup_inputs(seed: int = 0) -> dict:
    keys = jax.random.split(jax.random.key(seed), 22)
    hidden_in = draw_hidden_in(jax.random.fold_in(keys[21], 71), 0)
    state = scatter_about(keys[1], (BATCH, HEADS, HEAD, HEAD), 0.5, 3.0, ((0, 24), (1, 32)), jnp.float32)
    lower_bound = jnp.clip(0.05 + 0.9 * jax.random.uniform(keys[2], (HEADS, HEAD), jnp.float32) ** steps_of(keys[2], (HEADS, HEAD), ((0, 32),), -0.2, 0.2), 0.05, 0.95)
    w_forget = scatter_about(keys[3], (D, HD), D ** -0.5, 0.125, ((1, 32),))
    w_input = scatter_about(keys[4], (D, HD), D ** -0.5, 0.125, ((1, 32),))
    w_query = scatter_about(keys[5], (D, HD), D ** -0.5, 0.125, ((1, 32),))
    w_outgate = scatter_about(keys[6], (D, HD), D ** -0.5, 0.125, ((1, 32),))
    head_gain = jnp.clip(1.0 + 0.18 * jax.random.normal(keys[7], (HEAD,), jnp.float32), 0.1, 1.9)
    w_out = bell_draw_with(keys[8], (HD, D), HD ** -0.5, 0.1875, ((0, 32),), (0, 1, 32, 2.75))
    ln1_gain = draw_ln1_gain(jax.random.fold_in(keys[21], 71), 0)
    ln1_bias = scatter_about(keys[10], (D,), 0.3, 1.5, (), jnp.float32)
    routes_keys = jax.random.split(jax.random.fold_in(keys[11], 1), BATCH // SEQ_DEV)
    routes_turns = jax.random.permutation(jax.random.fold_in(keys[11], 3), BATCH // SEQ_DEV)
    routes = jax.vmap(lambda own, number: routed_block(jax.random.fold_in(keys[11], 2), own, number, SEQ_DEV, EXPERTS, TOPK, CAP, 2))(routes_keys, routes_turns).reshape((BATCH, TOPK))
    route_weights = jnp.clip(jnp.exp(math.log(1.5) - 2.014903 * jax.random.uniform(keys[12], (BATCH, TOPK), jnp.float32) ** steps_of(keys[12], (BATCH, TOPK), ((0, 24),), -0.2, 0.2)), 0.2, 1.5)
    exp_gate = scatter_about(keys[13], (EXPERTS, D, EFF), D ** -0.5, 0.125, ((0, 24), (2, 32)))
    exp_up = scatter_about(keys[14], (EXPERTS, D, EFF), D ** -0.5, 0.125, ((0, 24), (2, 32)))
    exp_down = bell_draw_with(keys[15], (EXPERTS, EFF, D), EFF ** -0.5, 0.1875, ((0, 24), (1, 32)), (1, 2, 32, 2.75))
    sh_gate = scatter_about(keys[16], (D, SFF), D ** -0.5, 0.125, ((1, 32),))
    sh_up = scatter_about(keys[17], (D, SFF), D ** -0.5, 0.125, ((1, 32),))
    sh_down = scatter_about(keys[18], (SFF, D), SFF ** -0.5, 0.25, ((0, 32),))
    ln2_gain = jnp.clip(1.0 + 0.18 * jax.random.normal(keys[19], (D,), jnp.float32), 0.1, 1.9)
    ln2_bias = scatter_about(keys[20], (D,), 0.3, 1.5, (), jnp.float32)
    return {"hidden_in": hidden_in, "state": state, "lower_bound": lower_bound, "w_forget": w_forget, "w_input": w_input, "w_query": w_query, "w_outgate": w_outgate, "head_gain": head_gain, "w_out": w_out, "ln1_gain": ln1_gain, "ln1_bias": ln1_bias, "routes": routes, "route_weights": route_weights, "exp_gate": exp_gate, "exp_up": exp_up, "exp_down": exp_down, "sh_gate": sh_gate, "sh_up": sh_up, "sh_down": sh_down, "ln2_gain": ln2_gain, "ln2_bias": ln2_bias}


EPS = 1e-05
ALPHA = 2.0 ** 0.25

def rounded(value):
    return lax.optimization_barrier(value.astype(jnp.bfloat16)).astype(jnp.float32)

def layer_norm(value, gain, bias):
    average = lax.optimization_barrier(jnp.mean(value, -1, keepdims=True))
    centered = value - average
    variance = lax.optimization_barrier(jnp.mean(centered * centered, -1, keepdims=True))
    return centered * lax.rsqrt(variance + EPS) * gain + bias

def reference(hidden_in, state, lower_bound, w_forget, w_input, w_query, w_outgate, head_gain, w_out, ln1_gain, ln1_bias, routes, route_weights, exp_gate, exp_up, exp_down, sh_gate, sh_up, sh_down, ln2_gain, ln2_bias):

    def project(weight):
        return rounded(jnp.dot(hidden_in, weight, preferred_element_type=jnp.float32)).reshape(BATCH, HEADS, HEAD)
    forget_pre = project(w_forget)
    forget = lower_bound + (1.0 - lower_bound) * jax.nn.sigmoid(forget_pre)
    key_part = (1.0 - lower_bound) * jax.nn.sigmoid(-forget_pre)
    values = project(w_input)
    queries = jax.nn.silu(project(w_query))
    out_gate = jax.nn.silu(project(w_outgate))
    new_state = forget[..., None] * state + key_part[..., None] * values[:, :, None, :]
    readout = jnp.einsum('bhd,bhdv->bhv', queries, new_state, precision=lax.Precision.HIGHEST)
    normed = readout * lax.rsqrt(lax.optimization_barrier(jnp.mean(readout * readout, -1, keepdims=True)) + EPS) * head_gain
    mixed = (normed * out_gate).astype(jnp.bfloat16).reshape(BATCH, -1)
    branch = jnp.dot(mixed, w_out, preferred_element_type=jnp.float32)
    normed_rows = layer_norm(ALPHA * hidden_in.astype(jnp.float32) + branch, ln1_gain, ln1_bias).astype(jnp.bfloat16)
    shared_hidden = (jax.nn.silu(jnp.dot(normed_rows, sh_gate, preferred_element_type=jnp.float32)) * jnp.dot(normed_rows, sh_up, preferred_element_type=jnp.float32)).astype(jnp.bfloat16)
    shared_out = jnp.dot(shared_hidden, sh_down, preferred_element_type=jnp.float32)
    routes_flat = routes.reshape(N_EP, SEQ_DEV * TOPK).astype(jnp.int32)
    one_hot = (routes_flat[..., None] == jnp.arange(EXPERTS, dtype=jnp.int32)[None, None, :]).astype(jnp.int32)
    position = lax.optimization_barrier(jnp.sum((jnp.cumsum(one_hot, 1) - one_hot) * one_hot, -1)).astype(jnp.int32)
    group_index = jnp.arange(N_EP, dtype=jnp.int32)[:, None]
    slot_index = (routes_flat * (N_EP * CAP) + group_index * CAP + position).reshape(-1).astype(jnp.int32)
    token_index = group_index * SEQ_DEV + jnp.arange(SEQ_DEV * TOPK, dtype=jnp.int32)[None, :] // TOPK
    token_index = token_index.reshape(-1).astype(jnp.int32)
    buffer = jnp.zeros((EXPERTS * N_EP * CAP, D), jnp.bfloat16).at[slot_index].set(normed_rows[token_index])
    buffer = buffer.reshape(EXPERTS, N_EP * CAP, D)
    block_width = EFF // N_TP

    def run_expert(operands):
        block_rows, gate_weight, up_weight, down_weight = operands
        gate_part = jnp.dot(block_rows, gate_weight, preferred_element_type=jnp.float32)
        up_part = jnp.dot(block_rows, up_weight, preferred_element_type=jnp.float32)
        hidden_part = (jax.nn.silu(gate_part) * up_part).astype(jnp.bfloat16)
        hidden_blocks = hidden_part.reshape(-1, N_TP, block_width).astype(jnp.float32)
        down_blocks = down_weight.reshape(N_TP, block_width, D).astype(jnp.float32)
        parts = jnp.einsum('snf,nfd->nsd', hidden_blocks, down_blocks)
        return lax.optimization_barrier(jnp.sum(rounded(parts), 0))
    outputs = lax.map(run_expert, (buffer, exp_gate, exp_up, exp_down)).reshape(-1, D)
    picked = outputs[slot_index].reshape(BATCH, TOPK, D)
    routed = lax.optimization_barrier(jnp.sum(route_weights[..., None] * picked, 1))
    result = layer_norm(ALPHA * normed_rows.astype(jnp.float32) + routed + shared_out, ln2_gain, ln2_bias)
    return (result.astype(jnp.bfloat16), new_state)
```

```python
import functools

import jax
import jax.numpy as jnp
from jax import lax
from jax.experimental import pallas as pl
from jax.experimental.pallas import tpu as pltpu
from jax.sharding import PartitionSpec as P

EPS = 1e-05
ALPHA = 2.0**0.25
MESH = pl.DeviceIdType.MESH
F32 = jnp.float32
BF16 = jnp.bfloat16
LANES = 128
HALF = 64

PH_HID, PH_MIX, PH_RS, PH_ROWS, PH_EP, PH_PICK, PH_OUT, PH_RET, PH_MOM = range(9)


def roll_half(x):
    return pltpu.roll(x, HALF, x.ndim - 1)


def low_lanes(shape):
    return lax.broadcasted_iota(jnp.int32, shape, len(shape) - 1) < HALF


def kernel(
    n_tp,
    n_ep,
    hid_ref,
    lb_ref,
    routes_ref,
    rw_ref,
    hg_ref,
    g1_ref,
    b1_ref,
    g1r_ref,
    b1r_ref,
    g2r_ref,
    b2r_ref,
    shg_ref,
    shu_ref,
    state_hbm,
    wf_hbm,
    wi_hbm,
    wq_hbm,
    wg_hbm,
    wout_hbm,
    eg_hbm,
    eu_hbm,
    ed_hbm,
    shd_ref,
    out_ref,
    f_ref,
    k_ref,
    v_ref,
    state,
    w4,
    wout,
    eg,
    eu,
    ed,
    s16,
    s128,
    hid_t,
    hid_all,
    mix_s,
    mix_r,
    rs_s,
    rs_r,
    row_t,
    row_all,
    ep_all,
    pick_t,
    pick_all,
    xrow,
    xnorm,
    out_s,
    out_r,
    ret_s,
    ret_r,
    mom_t,
    mom_all,
    lsem,
    ssem,
    rsem,
):
    g = lax.axis_index("ep")
    t = lax.axis_index("tp")
    pairs = n_tp // 2
    seq = hid_ref.shape[0]
    width = n_tp * HALF
    slot_rows = 2 * n_ep

    loads = [pltpu.make_async_copy(src, w4.at[i], lsem.at[i]) for i, src in enumerate((wf_hbm, wi_hbm, wq_hbm, wg_hbm))]
    loads.append(pltpu.make_async_copy(state_hbm, state, lsem.at[4]))
    loads.append(pltpu.make_async_copy(wout_hbm, wout, lsem.at[5]))
    loads.append(pltpu.make_async_copy(eg_hbm, eg, lsem.at[6]))
    loads.append(pltpu.make_async_copy(eu_hbm, eu, lsem.at[7]))
    loads.append(pltpu.make_async_copy(ed_hbm, ed, lsem.at[8]))
    for load in loads:
        load.start()

    barrier = pltpu.get_barrier_semaphore()

    def greet(axis, me, n):
        def body(i, c):
            pl.semaphore_signal(barrier, inc=1, device_id={axis: lax.rem(me + i, n)}, device_id_type=MESH)
            return c

        lax.fori_loop(1, n, body, 0)

    greet("ep", g, n_ep)
    greet("tp", t, n_tp)

    def send_tile(src, dst, axis, me, n, ph):
        def body(i, c):
            pltpu.make_async_remote_copy(
                src_ref=src,
                dst_ref=dst.at[me],
                send_sem=ssem.at[ph],
                recv_sem=rsem.at[ph],
                device_id={axis: lax.rem(me + i, n)},
                device_id_type=MESH,
            ).start()
            return c

        lax.fori_loop(1, n, body, 0)

    def send_tiles(src, dst, axis, me, n, ph):
        def body(i, c):
            p = lax.rem(me + i, n)
            pltpu.make_async_remote_copy(
                src_ref=src.at[p],
                dst_ref=dst.at[me],
                send_sem=ssem.at[ph],
                recv_sem=rsem.at[ph],
                device_id={axis: p},
                device_id_type=MESH,
            ).start()
            return c

        lax.fori_loop(1, n, body, 0)

    def whole(buf, axis, me, n, ph):
        part = buf.at[pl.ds(0, n - 1)]
        return pltpu.make_async_remote_copy(
            src_ref=part,
            dst_ref=part,
            send_sem=ssem.at[ph],
            recv_sem=rsem.at[ph],
            device_id={axis: lax.rem(me + 1, n)},
            device_id_type=MESH,
        )

    low8 = low_lanes((8, LANES))
    s16[...] = jnp.zeros_like(s16)
    s16[0:seq, 0:HALF] = hid_ref[...].astype(F32)
    hid_own = s16[0:8, :] + roll_half(s16[8:16, :])
    hid_t[...] = hid_own.astype(BF16)
    hid_all[t] = hid_own.astype(BF16)

    pl.semaphore_wait(barrier, n_ep + n_tp - 2)
    send_tile(hid_t, hid_all, "tp", t, n_tp, PH_HID)

    s128[...] = jnp.zeros_like(s128)
    s128[0:4, 0:seq] = routes_ref[...].astype(F32)
    s128[8:12, 0:seq] = rw_ref[...]
    by_row = jnp.transpose(s128[...])[0:16, :]
    lane16 = lax.broadcasted_iota(jnp.int32, (16, LANES), 1)
    row16 = lax.broadcasted_iota(jnp.int32, (16, LANES), 0)
    expert_of = (lane16 // 2).astype(F32)
    place_of = (lane16 % 2).astype(F32)
    named = jnp.zeros((16, LANES), F32)
    weight = jnp.zeros((16, LANES), F32)
    for k in range(4):
        hit = (by_row[:, k : k + 1] == expert_of) & (row16 < seq)
        named = named + jnp.where(hit, 1.0, 0.0)
        weight = weight + jnp.where(hit, by_row[:, 8 + k : 9 + k], 0.0)
    earlier = jnp.where(
        lax.broadcasted_iota(jnp.int32, (16, 16), 1) < lax.broadcasted_iota(jnp.int32, (16, 16), 0), 1.0, 0.0
    ).astype(BF16)
    before = jnp.dot(earlier, named.astype(BF16), preferred_element_type=F32)
    weight = jnp.where(before == place_of, weight, 0.0)
    first = (lane16 // 2) == g
    second = (lane16 // 2) == (n_ep + g)

    def mix_for(e, c):
        a = pltpu.roll(weight, lax.rem(2 * g - 4 * e + 4 * LANES, LANES), 1)
        b = pltpu.roll(weight, lax.rem(2 * n_ep + 2 * g - 4 * e - 2 + 4 * LANES, LANES), 1)
        mix_s[e] = jnp.where(first, a, jnp.where(second, b, 0.0)).reshape(2, 8, LANES)
        return c

    lax.fori_loop(0, n_ep, mix_for, 0)
    mix_r[g] = mix_s[g]
    send_tiles(mix_s, mix_r, "ep", g, n_ep, PH_MIX)

    def unfold(buf):
        left, right = [], []
        for p in range(pairs):
            a = buf[2 * p].astype(F32)
            b = buf[2 * p + 1].astype(F32)
            low = low_lanes(a.shape)
            left.append(jnp.where(low, a, roll_half(b)))
            right.append(jnp.where(low, roll_half(a), b))
        return left, right

    def full_rows(buf):
        left, right = unfold(buf)
        return jnp.concatenate([jnp.concatenate(left, 1), jnp.concatenate(right, 1)], 0)

    whole(hid_all, "tp", t, n_tp, PH_HID).wait_recv()
    rows = full_rows(hid_all).astype(BF16)

    def project(i):
        loads[i].wait()
        return jnp.dot(rows, w4[i], preferred_element_type=F32).astype(BF16).astype(F32)

    lower = lb_ref[...]
    forget_pre = project(0)
    forget = lower + (1.0 - lower) * jax.nn.sigmoid(forget_pre)
    key = (1.0 - lower) * jax.nn.sigmoid(-forget_pre)
    values = project(1)
    queries = project(2)
    queries = queries * jax.nn.sigmoid(queries)
    gate = project(3)
    gate = gate * jax.nn.sigmoid(gate)
    f_ref[...] = forget[0:seq]
    k_ref[...] = key[0:seq]
    v_ref[...] = values[0:seq]

    s128[0:16, :] = queries * forget
    by_channel = jnp.transpose(s128[...])
    loads[4].wait()
    for b in range(seq):
        s16[b : b + 1, :] = jnp.sum(by_channel[:, b : b + 1] * state[b], axis=0, keepdims=True)
    s16[seq:16, :] = jnp.zeros((16 - seq, LANES), F32)
    readout = s16[...] + jnp.sum(queries * key, axis=1, keepdims=True) * values
    mean_sq = jnp.mean(readout * readout, axis=1, keepdims=True)
    mixed = (readout * lax.rsqrt(mean_sq + EPS) * hg_ref[...] * gate).astype(BF16)

    def fold_out(top, bottom, p, buf, at, rows_of):
        low = low_lanes(top.shape)
        buf[2 * p, at : at + rows_of, :] = jnp.where(low, top, roll_half(bottom)).astype(BF16)
        buf[2 * p + 1, at : at + rows_of, :] = jnp.where(low, roll_half(top), bottom).astype(BF16)

    loads[5].wait()
    branch = jnp.dot(mixed, wout[...], preferred_element_type=F32)
    for p in range(pairs):
        block = branch[:, p * LANES : (p + 1) * LANES]
        fold_out(block[0:8], block[8:16], p, rs_s, 0, 8)
    rs_r[t] = rs_s[t]
    send_tiles(rs_s, rs_r, "tp", t, n_tp, PH_RS)

    whole(mix_r, "ep", g, n_ep, PH_MIX).wait_recv()
    mix_low = mix_r[:, 0].reshape(n_ep * 8, LANES)
    mix_high = mix_r[:, 1].reshape(n_ep * 8, LANES)
    pick_low = jnp.where(mix_low != 0.0, 1.0, 0.0).astype(BF16)
    pick_high = jnp.where(mix_high != 0.0, 1.0, 0.0).astype(BF16)

    whole(rs_r, "tp", t, n_tp, PH_RS).wait_recv()
    own = ALPHA * hid_own + jnp.sum(rs_r[...].astype(F32), axis=0)
    row_t[...] = own.astype(BF16)
    row_all[t] = own.astype(BF16)
    ep_all[g] = own.astype(BF16)
    send_tile(row_t, ep_all, "ep", g, n_ep, PH_EP)
    send_tile(row_t, row_all, "tp", t, n_tp, PH_ROWS)

    over_rows = (((0,), (0,)), ((), ()))
    whole(ep_all, "ep", g, n_ep, PH_EP).wait_recv()
    tiles = ep_all[...].astype(F32).reshape(n_ep * 8, LANES).astype(BF16)
    got_low = lax.dot_general(pick_low, tiles, over_rows, preferred_element_type=F32)
    got_high = lax.dot_general(pick_high, tiles, over_rows, preferred_element_type=F32)
    low_s = low_lanes((slot_rows, LANES))
    one, two = slice(0, slot_rows), slice(slot_rows, 2 * slot_rows)
    picked = jnp.where(
        low_s,
        got_low[one] + roll_half(got_high[one]),
        roll_half(got_low[two]) + got_high[two],
    ).astype(BF16)
    pick_t[...] = picked
    pick_all[t] = picked
    send_tile(pick_t, pick_all, "tp", t, n_tp, PH_PICK)

    whole(row_all, "tp", t, n_tp, PH_ROWS).wait_recv()
    full = full_rows(row_all)
    mean1 = jnp.mean(full, axis=1, keepdims=True)
    centred = full - mean1
    rstd1 = lax.rsqrt(jnp.mean(centred * centred, axis=1, keepdims=True) + EPS)
    normed = (centred * rstd1 * g1_ref[...] + b1_ref[...]).astype(BF16)
    over_cols = (((1,), (1,)), ((), ()))
    sh_gate = lax.dot_general(normed, shg_ref[...], over_cols, preferred_element_type=F32)
    sh_up = lax.dot_general(normed, shu_ref[...], over_cols, preferred_element_type=F32)
    sh_hidden = (sh_gate * jax.nn.sigmoid(sh_gate) * sh_up).astype(BF16)
    shared = jnp.dot(sh_hidden, shd_ref[...], preferred_element_type=F32)
    for p in range(pairs):
        block = shared[:, p * LANES : (p + 1) * LANES]
        fold_out(block[0:8], block[8:16], p, out_s, slot_rows, 8)

    def own_columns(ref):
        row = jnp.broadcast_to(ref[pl.ds(t // 2, 1), :], (8, LANES))
        swapped = roll_half(row)
        even = lax.rem(t, 2) == 0
        return jnp.where(low8, jnp.where(even, row, swapped), jnp.where(even, swapped, row))

    def fold_rows(col):
        return jnp.where(low8, col[0:8], col[8:16])

    own_normed = ((own - fold_rows(mean1)) * fold_rows(rstd1) * own_columns(g1r_ref) + own_columns(b1r_ref)).astype(
        BF16
    ).astype(F32)

    whole(pick_all, "tp", t, n_tp, PH_PICK).wait_recv()
    sums = [jnp.zeros((slot_rows, LANES), F32), jnp.zeros((slot_rows, LANES), F32)]
    for p in range(pairs):
        a = pick_all[2 * p].astype(F32)
        b = pick_all[2 * p + 1].astype(F32)
        cols = slice(p * LANES, (p + 1) * LANES)
        x0 = jnp.where(low_s, a, roll_half(b))
        x1 = jnp.where(low_s, roll_half(a), b)
        xrow[one, cols] = x0
        xrow[two, cols] = x1
        sums = [sums[0] + x0, sums[1] + x1]
    for j, rows_j in enumerate((one, two)):
        mean = jnp.sum(sums[j], axis=1, keepdims=True) / width
        total = jnp.zeros((slot_rows, LANES), F32)
        for p in range(pairs):
            d = xrow[rows_j, p * LANES : (p + 1) * LANES] - mean
            total = total + d * d
        rstd = lax.rsqrt(jnp.sum(total, axis=1, keepdims=True) / width + EPS)
        for p in range(pairs):
            cols = slice(p * LANES, (p + 1) * LANES)
            xnorm[rows_j, cols] = (
                (xrow[rows_j, cols] - mean) * rstd * g1_ref[:, cols] + b1_ref[:, cols]
            ).astype(BF16)
    for i in (6, 7):
        loads[i].wait()
    hidden = []
    for j, rows_j in enumerate((one, two)):
        gate_j = jnp.dot(xnorm[rows_j, :], eg[j], preferred_element_type=F32)
        up_j = jnp.dot(xnorm[rows_j, :], eu[j], preferred_element_type=F32)
        hidden.append((gate_j * jax.nn.sigmoid(gate_j) * up_j).astype(BF16))
    loads[8].wait()
    step = min(256, width)
    for n in range(width // step):
        cols = slice(n * step, (n + 1) * step)
        y0 = jnp.dot(hidden[0], ed[0, :, cols], preferred_element_type=F32)
        y1 = jnp.dot(hidden[1], ed[1, :, cols], preferred_element_type=F32)
        for q in range(step // LANES):
            sub = slice(q * LANES, (q + 1) * LANES)
            fold_out(y0[:, sub], y1[:, sub], n * (step // LANES) + q, out_s, 0, slot_rows)
    out_r[t] = out_s[t]
    send_tiles(out_s, out_r, "tp", t, n_tp, PH_OUT)

    whole(out_r, "tp", t, n_tp, PH_OUT).wait_recv()
    summed = jnp.sum(out_r[...].astype(F32), axis=0)
    slots = summed[0:slot_rows]
    turned = roll_half(slots)
    both = jnp.concatenate([jnp.where(low_s, slots, turned), jnp.where(low_s, turned, slots)], 0)
    used = 2 * slot_rows
    back_low = jnp.dot(mix_low[:, 0:used], both, precision=lax.Precision.HIGHEST, preferred_element_type=F32)
    back_high = jnp.dot(mix_high[:, 0:used], both, precision=lax.Precision.HIGHEST, preferred_element_type=F32)
    back = jnp.where(low_lanes((n_ep * 8, LANES)), back_low, back_high)
    ret_s[...] = back.reshape(n_ep, 8, LANES).astype(BF16)
    ret_r[g] = ret_s[g]
    send_tiles(ret_s, ret_r, "ep", g, n_ep, PH_RET)
    whole(ret_r, "ep", g, n_ep, PH_RET).wait_recv()
    final = ALPHA * own_normed + jnp.sum(ret_r[...].astype(F32), axis=0) + summed[slot_rows : slot_rows + 8]

    mine = jnp.concatenate([jnp.where(low8, final, 0.0), jnp.where(low8, roll_half(final), 0.0)], 0)
    part = jnp.where(lane16 == row16, jnp.sum(mine, axis=1, keepdims=True), 0.0) + jnp.where(
        lane16 == row16 + 16, jnp.sum(mine * mine, axis=1, keepdims=True), 0.0
    )
    part = jnp.sum(part, axis=0, keepdims=True)
    mom_t[...] = part
    mom_all[t] = part
    send_tile(mom_t, mom_all, "tp", t, n_tp, PH_MOM)
    whole(mom_all, "tp", t, n_tp, PH_MOM).wait_recv()
    moments = jnp.broadcast_to(jnp.sum(mom_all[...], axis=0) / width, (16, LANES))
    mean2 = jnp.sum(jnp.where(lane16 == row16, moments, 0.0), axis=1, keepdims=True)
    square2 = jnp.sum(jnp.where(lane16 == row16 + 16, moments, 0.0), axis=1, keepdims=True)
    rstd2 = lax.rsqrt(square2 - mean2 * mean2 + EPS)
    done = (final - fold_rows(mean2)) * fold_rows(rstd2) * own_columns(g2r_ref) + own_columns(b2r_ref)
    s16[0:8, :] = done
    s16[8:16, :] = roll_half(done)
    out_ref[...] = s16[0:seq, 0:HALF].astype(BF16)

    for buf, axis, me, n, ph in (
        (hid_all, "tp", t, n_tp, PH_HID),
        (mix_r, "ep", g, n_ep, PH_MIX),
        (rs_r, "tp", t, n_tp, PH_RS),
        (row_all, "tp", t, n_tp, PH_ROWS),
        (ep_all, "ep", g, n_ep, PH_EP),
        (pick_all, "tp", t, n_tp, PH_PICK),
        (out_r, "tp", t, n_tp, PH_OUT),
        (ret_r, "ep", g, n_ep, PH_RET),
        (mom_all, "tp", t, n_tp, PH_MOM),
    ):
        whole(buf, axis, me, n, ph).wait_send()


def local(
    hidden_in,
    state,
    lower_bound,
    w_forget,
    w_input,
    w_query,
    w_outgate,
    head_gain,
    w_out,
    ln1_gain,
    ln1_bias,
    routes,
    route_weights,
    exp_gate,
    exp_up,
    exp_down,
    sh_gate,
    sh_up,
    sh_down,
    ln2_gain,
    ln2_bias,
):
    n_tp = lax.axis_size("tp")
    n_ep = lax.axis_size("ep")
    seq = hidden_in.shape[0]
    width = w_forget.shape[0]
    slot_rows = 2 * n_ep
    vmem = pl.BlockSpec(memory_space=pltpu.VMEM)
    hbm = pl.BlockSpec(memory_space=pltpu.HBM)
    sem = pltpu.SemaphoreType.DMA
    small = jax.ShapeDtypeStruct((seq, LANES), F32)
    state3 = state.reshape(seq, LANES, LANES)
    mixed_out, forget, key, values = pl.pallas_call(
        functools.partial(kernel, n_tp, n_ep),
        out_shape=(jax.ShapeDtypeStruct(hidden_in.shape, BF16), small, small, small),
        in_specs=[vmem] * 13 + [hbm] * 9 + [vmem],
        out_specs=(vmem,) * 4,
        scratch_shapes=[
            pltpu.VMEM((seq, LANES, LANES), F32),
            pltpu.VMEM((4, width, LANES), BF16),
            pltpu.VMEM((LANES, width), BF16),
            pltpu.VMEM((2, width, LANES), BF16),
            pltpu.VMEM((2, width, LANES), BF16),
            pltpu.VMEM((2, LANES, width), BF16),
            pltpu.VMEM((16, LANES), F32),
            pltpu.VMEM((LANES, LANES), F32),
            pltpu.VMEM((8, LANES), BF16),
            pltpu.VMEM((n_tp, 8, LANES), BF16),
            pltpu.VMEM((n_ep, 2, 8, LANES), F32),
            pltpu.VMEM((n_ep, 2, 8, LANES), F32),
            pltpu.VMEM((n_tp, 8, LANES), BF16),
            pltpu.VMEM((n_tp, 8, LANES), BF16),
            pltpu.VMEM((8, LANES), BF16),
            pltpu.VMEM((n_tp, 8, LANES), BF16),
            pltpu.VMEM((n_ep, 8, LANES), BF16),
            pltpu.VMEM((slot_rows, LANES), BF16),
            pltpu.VMEM((n_tp, slot_rows, LANES), BF16),
            pltpu.VMEM((2 * slot_rows, width), F32),
            pltpu.VMEM((2 * slot_rows, width), BF16),
            pltpu.VMEM((n_tp, slot_rows + 8, LANES), BF16),
            pltpu.VMEM((n_tp, slot_rows + 8, LANES), BF16),
            pltpu.VMEM((n_ep, 8, LANES), BF16),
            pltpu.VMEM((n_ep, 8, LANES), BF16),
            pltpu.VMEM((1, LANES), F32),
            pltpu.VMEM((n_tp, 1, LANES), F32),
            sem((9,)),
            sem((9,)),
            sem((9,)),
        ],
        compiler_params=pltpu.CompilerParams(collective_id=0, has_side_effects=True),
        name="decode_step",
    )(
        hidden_in,
        lower_bound,
        routes.T,
        route_weights.T,
        head_gain.reshape(1, LANES),
        ln1_gain.reshape(1, width),
        ln1_bias.reshape(1, width),
        ln1_gain.reshape(width // LANES, LANES),
        ln1_bias.reshape(width // LANES, LANES),
        ln2_gain.reshape(width // LANES, LANES),
        ln2_bias.reshape(width // LANES, LANES),
        sh_gate.T,
        sh_up.T,
        state3,
        w_forget,
        w_input,
        w_query,
        w_outgate,
        w_out,
        exp_gate,
        exp_up,
        exp_down,
        sh_down,
    )
    new_state = forget[:, :, None] * state3 + key[:, :, None] * values[:, None, :]
    return (mixed_out, new_state.reshape(state.shape))


def solution(mesh):
    placed = (
        P("ep", "tp"),
        P("ep", "tp", None, None),
        P("tp", None),
        P(None, "tp"),
        P(None, "tp"),
        P(None, "tp"),
        P(None, "tp"),
        P(),
        P("tp", None),
        P(),
        P(),
        P("ep", None),
        P("ep", None),
        P("ep", None, "tp"),
        P("ep", None, "tp"),
        P("ep", "tp", None),
        P(None, "tp"),
        P(None, "tp"),
        P("tp", None),
        P(),
        P(),
    )
    return jax.shard_map(
        local,
        mesh=mesh,
        in_specs=placed,
        out_specs=(P("ep", "tp"), P("ep", "tp", None, None)),
        check_vma=False,
    )
```

```python
import functools

import jax
import jax.numpy as jnp
from jax import lax
from jax.experimental import pallas as pl
from jax.experimental.pallas import tpu as pltpu
from jax.sharding import PartitionSpec as P

EPS = 1e-05
ALPHA = 2.0**0.25
MESH = pl.DeviceIdType.MESH
F32 = jnp.float32
BF16 = jnp.bfloat16
LANES = 128
HALF = 64

PH_HID, PH_MIX, PH_RS, PH_ROWS, PH_RET, PH_MOM, PH_SH, PH_EP, PH_PICK, PH_OUT = 0, 1, 2, 3, 4, 5, 6, 7, 10, 13
N_PH = 16
CLASSES = 3


def roll_half(x):
    return pltpu.roll(x, HALF, x.ndim - 1)


def low_lanes(shape):
    return lax.broadcasted_iota(jnp.int32, shape, len(shape) - 1) < HALF


def spread(k):
    return ((k + 1) // 2) * (2 * lax.rem(k, 2) - 1)


def kernel(n_tp, n_ep, n_x, *refs):
    hbm, refs = refs[:23], refs[23:]
    (out_ref, ns_hbm), refs = refs[:2], refs[2:]
    vm, refs = refs[:23], refs[23:]
    (
        s16,
        s128,
        hid_t,
        hid_all,
        mix_s,
        mix_r,
        mix_low,
        mix_high,
        choose,
        rs_s,
        rs_r,
        row_t,
        row_all,
        ep_all,
        pick_t,
        pick_all,
        xrow,
        xnorm,
        sh_s,
        sh_r,
        out_s,
        out_r,
        ret_s,
        ret_r,
        mom_t,
        mom_all,
        lsem,
        ssem,
        rsem,
    ) = refs
    (
        hid_ref,
        routes_ref,
        rw_ref,
        wf,
        wi,
        wq,
        wg,
        lb_ref,
        hg_ref,
        state,
        wout,
        g1_ref,
        b1_ref,
        shg_ref,
        shu_ref,
        shd_ref,
        g1r_ref,
        b1r_ref,
        egu,
        ed,
        g2r_ref,
        b2r_ref,
    ) = vm[:22]
    egu_extra = hbm[22]

    g = lax.axis_index("ep")
    t = lax.axis_index("tp")
    core = lax.rem(g, 2)
    z = g // 2
    n_z = n_ep // 2
    n_y = n_tp // n_x
    y = t // n_x
    x = lax.rem(t, n_x)
    pairs = n_tp // 2
    seq = hid_ref.shape[0]
    width = n_tp * HALF
    per_class = n_ep // CLASSES
    rows_j = 2 * per_class

    barrier = pltpu.get_barrier_semaphore()

    def tp_peer(i):
        dy = n_y // 2 + spread(i // n_x)
        dx = n_x // 2 + spread(lax.rem(i, n_x))
        return lax.rem(y + dy, n_y) * n_x + lax.rem(x + dx, n_x)

    def ep_peer(i):
        k = (n_z - 1) - i // 2
        to_core = lax.rem(core + 1 + lax.rem(i, 2), 2)
        chip = lax.rem(z + n_z - spread(k), n_z)
        return k, 2 * chip + to_core

    def greet_tp(i, c):
        pl.semaphore_signal(barrier, inc=1, device_id={"tp": tp_peer(i)}, device_id_type=MESH)
        return c

    def greet_ep(i, c):
        pl.semaphore_signal(barrier, inc=1, device_id={"ep": ep_peer(i)[1]}, device_id_type=MESH)
        return c

    lax.fori_loop(0, n_tp - 1, greet_tp, 0)
    lax.fori_loop(0, n_ep - 1, greet_ep, 0)

    loads = []
    for i in range(22):
        if i == 18:
            loads.append(
                [
                    pltpu.make_async_copy(hbm[i], egu.at[:, :, 0:LANES], lsem.at[i]),
                    pltpu.make_async_copy(egu_extra, egu.at[:, :, LANES : 2 * LANES], lsem.at[22]),
                ]
            )
        else:
            loads.append([pltpu.make_async_copy(hbm[i], vm[i], lsem.at[i])])
    for group in loads:
        for load in group:
            load.start()

    def ready(*which):
        for i in which:
            for load in loads[i]:
                load.wait()

    def remote(src, dst, ph, device):
        return pltpu.make_async_remote_copy(
            src_ref=src,
            dst_ref=dst,
            send_sem=ssem.at[ph],
            recv_sem=rsem.at[ph],
            device_id=device,
            device_id_type=MESH,
        )

    def tp_tile(src, dst, ph):
        def body(i, c):
            remote(src, dst.at[t], ph, {"tp": tp_peer(i)}).start()
            return c

        lax.fori_loop(0, n_tp - 1, body, 0)

    def tp_tiles(src, dst, ph):
        def body(i, c):
            p = tp_peer(i)
            remote(src.at[p], dst.at[t], ph, {"tp": p}).start()
            return c

        lax.fori_loop(0, n_tp - 1, body, 0)

    def whole(buf, count, ph):
        part = buf.at[pl.ds(0, count)]
        return remote(part, part, ph, {"tp": tp_peer(0)})

    low8 = low_lanes((8, LANES))
    s16[...] = jnp.zeros_like(s16)
    ready(0)
    s16[0:seq, 0:HALF] = hid_ref[...].astype(F32)
    hid_own = s16[0:8, :] + roll_half(s16[8:16, :])
    hid_t[...] = hid_own.astype(BF16)
    hid_all[t] = hid_own.astype(BF16)

    pl.semaphore_wait(barrier, n_ep + n_tp - 2)
    tp_tile(hid_t, hid_all, PH_HID)

    ready(1, 2)
    s128[...] = jnp.zeros_like(s128)
    s128[0:4, 0:seq] = routes_ref[...].astype(F32)
    s128[8:12, 0:seq] = rw_ref[...]
    by_row = jnp.transpose(s128[...])[0:16, :]
    lane16 = lax.broadcasted_iota(jnp.int32, (16, LANES), 1)
    row16 = lax.broadcasted_iota(jnp.int32, (16, LANES), 0)
    expert_of = (lane16 // 2).astype(F32)
    place_of = (lane16 % 2).astype(F32)
    named = jnp.zeros((16, LANES), F32)
    weight = jnp.zeros((16, LANES), F32)
    for k in range(4):
        hit = (by_row[:, k : k + 1] == expert_of) & (row16 < seq)
        named = named + jnp.where(hit, 1.0, 0.0)
        weight = weight + jnp.where(hit, by_row[:, 8 + k : 9 + k], 0.0)
    earlier = jnp.where(
        lax.broadcasted_iota(jnp.int32, (16, 16), 1) < lax.broadcasted_iota(jnp.int32, (16, 16), 0), 1.0, 0.0
    ).astype(BF16)
    before = jnp.dot(earlier, named.astype(BF16), preferred_element_type=F32)
    weight = jnp.where(before == place_of, weight, 0.0)
    s128[...] = jnp.zeros_like(s128)
    s128[0:16, :] = weight
    by_code = jnp.transpose(s128[...])
    lane32 = lax.broadcasted_iota(jnp.int32, (32, LANES), 1)
    row32 = lax.broadcasted_iota(jnp.int32, (32, LANES), 0)
    message = jnp.zeros((32, LANES), F32)
    for c in range(4):
        take = jnp.where(lane32 == 4 * row32 + c, 1.0, 0.0)
        part = jnp.dot(take, by_code, precision=lax.Precision.HIGHEST, preferred_element_type=F32)
        message = message + (part if c == 0 else pltpu.roll(part, 16 * c, 1))
    for e in range(n_ep):
        mix_s[e] = message[e : e + 1, :]
    mix_r[core] = mix_s[g]

    def mix_send(i, c):
        k, e = ep_peer(i)
        remote(mix_s.at[e], mix_r.at[2 * k + core], PH_MIX, {"ep": e}).start()
        return c

    lax.fori_loop(0, n_ep - 1, mix_send, 0)

    def full_rows(buf):
        left, right = [], []
        for p in range(pairs):
            a = buf[2 * p].astype(F32)
            b = buf[2 * p + 1].astype(F32)
            left.append(jnp.where(low8, a, roll_half(b)))
            right.append(jnp.where(low8, roll_half(a), b))
        return jnp.concatenate([jnp.concatenate(left, 1), jnp.concatenate(right, 1)], 0)

    whole(hid_all, n_tp - 1, PH_HID).wait_recv()
    rows = full_rows(hid_all).astype(BF16)

    def project(i):
        ready(i)
        return jnp.dot(rows, vm[i][...], preferred_element_type=F32).astype(BF16).astype(F32)

    forget_pre = project(3)
    values = project(4)
    queries = project(5)
    queries = queries * jax.nn.sigmoid(queries)
    gate = project(6)
    gate = gate * jax.nn.sigmoid(gate)
    ready(7, 8)
    lower = lb_ref[...]
    forget = lower + (1.0 - lower) * jax.nn.sigmoid(forget_pre)
    key = (1.0 - lower) * jax.nn.sigmoid(-forget_pre)

    s128[0:16, :] = queries * forget
    by_channel = jnp.transpose(s128[...])
    ready(9)
    for b in range(seq):
        s16[b : b + 1, :] = jnp.sum(by_channel[:, b : b + 1] * state[b], axis=0, keepdims=True)
    s16[seq:16, :] = jnp.zeros((16 - seq, LANES), F32)
    readout = s16[...] + jnp.sum(queries * key, axis=1, keepdims=True) * values
    mean_sq = jnp.mean(readout * readout, axis=1, keepdims=True)
    mixed = (readout * lax.rsqrt(mean_sq + EPS) * hg_ref[...] * gate).astype(BF16)

    def fold_out(top, bottom, p, buf):
        low = low_lanes(top.shape)
        buf[2 * p] = jnp.where(low, top, roll_half(bottom)).astype(BF16)
        buf[2 * p + 1] = jnp.where(low, roll_half(top), bottom).astype(BF16)

    ready(10)
    branch = jnp.dot(mixed, wout[...], preferred_element_type=F32)
    for p in range(pairs):
        block = branch[:, p * LANES : (p + 1) * LANES]
        fold_out(block[0:8], block[8:16], p, rs_s)
    rs_r[t] = rs_s[t]
    tp_tiles(rs_s, rs_r, PH_RS)

    s128[0:16, :] = forget
    forget_col = jnp.transpose(s128[...])
    s128[0:16, :] = key
    key_col = jnp.transpose(s128[...])
    for b in range(seq):
        state[b] = forget_col[:, b : b + 1] * state[b] + key_col[:, b : b + 1] * values[b : b + 1, :]

    whole(mix_r, n_ep - 1, PH_MIX).wait_recv()
    lane8 = lax.broadcasted_iota(jnp.int32, (8, LANES), 1)
    row8 = lax.broadcasted_iota(jnp.int32, (8, LANES), 0)
    mask_low = (lane8 < HALF) & (lane8 % 16 == row8)
    mask_high = (lane8 < HALF) & (lane8 % 16 == row8 + 8)
    every = [jnp.broadcast_to(mix_r[r], (8, LANES)) for r in range(n_ep)]
    from_lane = lax.broadcasted_iota(jnp.int32, (LANES, LANES), 0)
    to_lane = lax.broadcasted_iota(jnp.int32, (LANES, LANES), 1)
    place = jnp.where(
        (from_lane < HALF) & (to_lane == (from_lane // 32) * rows_j + (from_lane // 16) % 2), 1.0, 0.0
    )
    for mask, keep in ((mask_low, mix_low), (mask_high, mix_high)):
        stacked = jnp.concatenate([jnp.where(mask, row, 0.0) for row in every], 0)
        placed = jnp.dot(stacked, place, precision=lax.Precision.HIGHEST, preferred_element_type=F32)
        for r in range(n_ep):
            at = 2 * (r % per_class)
            piece = placed[8 * r : 8 * r + 8]
            keep[r] = piece if at == 0 else pltpu.roll(piece, at, 1)
    for c in range(CLASSES):
        part = slice(c * per_class, (c + 1) * per_class)
        low_c = jnp.where(mix_low[part].reshape(8 * per_class, LANES) != 0.0, 1.0, 0.0)
        high_c = jnp.where(mix_high[part].reshape(8 * per_class, LANES) != 0.0, 1.0, 0.0)
        s128[0 : 8 * per_class, :] = low_c + pltpu.roll(high_c, 2 * rows_j, 1)
        choose[c] = jnp.transpose(s128[...])[0 : 4 * rows_j, 0 : 8 * per_class].astype(BF16)

    whole(rs_r, n_tp - 1, PH_RS).wait_recv()
    own = ALPHA * hid_own + jnp.sum(rs_r[...].astype(F32), axis=0)
    row_t[...] = own.astype(BF16)
    row_all[t] = own.astype(BF16)
    ep_all[core] = own.astype(BF16)

    def ep_send(i, c):
        k, e = ep_peer(i)
        remote(row_t, ep_all.at[2 * k + core], PH_EP + (2 * k) // per_class, {"ep": e}).start()
        return c

    lax.fori_loop(0, n_ep - 1, ep_send, 0)
    tp_tile(row_t, row_all, PH_ROWS)
    store = pltpu.make_async_copy(state, ns_hbm, lsem.at[23])
    store.start()

    low_j = low_lanes((rows_j, LANES))
    one, two = slice(0, rows_j), slice(rows_j, 2 * rows_j)
    for c in range(CLASSES):
        whole(ep_all, per_class - 1 if c == 0 else per_class, PH_EP + c).wait_recv()
        tiles = ep_all[c * per_class : (c + 1) * per_class].astype(F32).reshape(8 * per_class, LANES).astype(BF16)
        got = jnp.dot(choose[c], tiles, preferred_element_type=F32)
        got_low, got_high = got[0 : 2 * rows_j], got[2 * rows_j : 4 * rows_j]
        picked = jnp.where(
            low_j,
            got_low[one] + roll_half(got_high[one]),
            roll_half(got_low[two]) + got_high[two],
        ).astype(BF16)
        pick_t[c] = picked
        pick_all[c, t] = picked
        tp_tile(pick_t.at[c], pick_all.at[c], PH_PICK + c)

    ready(11, 12, 13, 14, 15, 16, 17)
    whole(row_all, n_tp - 1, PH_ROWS).wait_recv()
    full = full_rows(row_all)
    mean1 = jnp.mean(full, axis=1, keepdims=True)
    centred = full - mean1
    rstd1 = lax.rsqrt(jnp.mean(centred * centred, axis=1, keepdims=True) + EPS)
    normed = (centred * rstd1 * g1_ref[...] + b1_ref[...]).astype(BF16)
    over_cols = (((1,), (1,)), ((), ()))
    sh_gate = lax.dot_general(normed, shg_ref[...], over_cols, preferred_element_type=F32)
    sh_up = lax.dot_general(normed, shu_ref[...], over_cols, preferred_element_type=F32)
    sh_hidden = (sh_gate * jax.nn.sigmoid(sh_gate) * sh_up).astype(BF16)
    shared = jnp.dot(sh_hidden, shd_ref[...], preferred_element_type=F32)
    for p in range(pairs):
        block = shared[:, p * LANES : (p + 1) * LANES]
        fold_out(block[0:8], block[8:16], p, sh_s)

    def own_columns(ref):
        row = jnp.broadcast_to(ref[pl.ds(t // 2, 1), :], (8, LANES))
        swapped = roll_half(row)
        even = lax.rem(t, 2) == 0
        return jnp.where(low8, jnp.where(even, row, swapped), jnp.where(even, swapped, row))

    def fold_rows(col):
        return jnp.where(low8, col[0:8], col[8:16])

    own_normed = ((own - fold_rows(mean1)) * fold_rows(rstd1) * own_columns(g1r_ref) + own_columns(b1r_ref)).astype(
        BF16
    ).astype(F32)

    ready(18, 19)
    for c in range(CLASSES):
        whole(pick_all.at[c], n_tp - 1, PH_PICK + c).wait_recv()
        sums = [jnp.zeros((rows_j, LANES), F32), jnp.zeros((rows_j, LANES), F32)]
        for p in range(pairs):
            a = pick_all[c, 2 * p].astype(F32)
            b = pick_all[c, 2 * p + 1].astype(F32)
            cols = slice(p * LANES, (p + 1) * LANES)
            x0 = jnp.where(low_j, a, roll_half(b))
            x1 = jnp.where(low_j, roll_half(a), b)
            xrow[one, cols] = x0
            xrow[two, cols] = x1
            sums = [sums[0] + x0, sums[1] + x1]
        hidden = []
        for j, at in enumerate((one, two)):
            mean = jnp.sum(sums[j], axis=1, keepdims=True) / width
            total = jnp.zeros((rows_j, LANES), F32)
            for p in range(pairs):
                d = xrow[at, p * LANES : (p + 1) * LANES] - mean
                total = total + d * d
            rstd = lax.rsqrt(jnp.sum(total, axis=1, keepdims=True) / width + EPS)
            for p in range(pairs):
                cols = slice(p * LANES, (p + 1) * LANES)
                xnorm[at, cols] = ((xrow[at, cols] - mean) * rstd * g1_ref[:, cols] + b1_ref[:, cols]).astype(BF16)
            both = jnp.dot(xnorm[at, :], egu[j], preferred_element_type=F32)
            gate_j, up_j = both[:, 0:LANES], both[:, LANES : 2 * LANES]
            hidden.append((gate_j * jax.nn.sigmoid(gate_j) * up_j).astype(BF16))
        step = min(256, width)
        for n in range(width // step):
            cols = slice(n * step, (n + 1) * step)
            y0 = jnp.dot(hidden[0], ed[0, :, cols], preferred_element_type=F32)
            y1 = jnp.dot(hidden[1], ed[1, :, cols], preferred_element_type=F32)
            for q in range(step // LANES):
                sub = slice(q * LANES, (q + 1) * LANES)
                fold_out(y0[:, sub], y1[:, sub], n * (step // LANES) + q, out_s.at[c])
        out_r[c, t] = out_s[c, t]
        tp_tiles(out_s.at[c], out_r.at[c], PH_OUT + c)
        if c == 0:
            sh_r[t] = sh_s[t]
            tp_tiles(sh_s, sh_r, PH_SH)

    for c in range(CLASSES):
        whole(out_r.at[c], n_tp - 1, PH_OUT + c).wait_recv()
        slots = jnp.sum(out_r[c].astype(F32), axis=0)
        turned = roll_half(slots)
        both = jnp.concatenate([jnp.where(low_j, slots, turned), jnp.where(low_j, turned, slots)], 0)
        part = slice(c * per_class, (c + 1) * per_class)
        low_c = mix_low[part].reshape(8 * per_class, LANES)[:, 0 : 2 * rows_j]
        high_c = mix_high[part].reshape(8 * per_class, LANES)[:, 0 : 2 * rows_j]
        back_low = jnp.dot(low_c, both, precision=lax.Precision.HIGHEST, preferred_element_type=F32)
        back_high = jnp.dot(high_c, both, precision=lax.Precision.HIGHEST, preferred_element_type=F32)
        back = jnp.where(low_lanes((8 * per_class, LANES)), back_low, back_high)
        ret_s[part] = back.reshape(per_class, 8, LANES).astype(BF16)
        if c == 0:
            ret_r[g] = ret_s[core]

        def ret_send(i, carry, c=c):
            r = c * per_class + i
            chip = lax.rem(z + n_z + spread(r // 2), n_z)
            e = 2 * chip + lax.rem(r, 2)

            @pl.when(e != g)
            def _():
                remote(ret_s.at[r], ret_r.at[g], PH_RET, {"ep": e}).start()

            return carry

        lax.fori_loop(0, per_class, ret_send, 0)

    ready(20, 21)
    whole(sh_r, n_tp - 1, PH_SH).wait_recv()
    final = ALPHA * own_normed + jnp.sum(sh_r[...].astype(F32), axis=0)
    whole(ret_r, n_ep - 1, PH_RET).wait_recv()
    final = final + jnp.sum(ret_r[...].astype(F32), axis=0)

    mine = jnp.concatenate([jnp.where(low8, final, 0.0), jnp.where(low8, roll_half(final), 0.0)], 0)
    part = jnp.where(lane16 == row16, jnp.sum(mine, axis=1, keepdims=True), 0.0) + jnp.where(
        lane16 == row16 + 16, jnp.sum(mine * mine, axis=1, keepdims=True), 0.0
    )
    part = jnp.sum(part, axis=0, keepdims=True)
    mom_t[...] = part
    mom_all[t] = part
    tp_tile(mom_t, mom_all, PH_MOM)
    store.wait()
    for buf, count, ph in (
        (hid_all, n_tp - 1, PH_HID),
        (mix_r, n_ep - 1, PH_MIX),
        (rs_r, n_tp - 1, PH_RS),
        (row_all, n_tp - 1, PH_ROWS),
        (sh_r, n_tp - 1, PH_SH),
        (ret_r, n_ep - 1, PH_RET),
    ):
        whole(buf, count, ph).wait_send()
    for c in range(CLASSES):
        whole(ep_all, per_class - 1 if c == 0 else per_class, PH_EP + c).wait_send()
        whole(pick_all.at[c], n_tp - 1, PH_PICK + c).wait_send()
        whole(out_r.at[c], n_tp - 1, PH_OUT + c).wait_send()
    whole(mom_all, n_tp - 1, PH_MOM).wait_recv()
    moments = jnp.broadcast_to(jnp.sum(mom_all[...], axis=0) / width, (16, LANES))
    mean2 = jnp.sum(jnp.where(lane16 == row16, moments, 0.0), axis=1, keepdims=True)
    square2 = jnp.sum(jnp.where(lane16 == row16 + 16, moments, 0.0), axis=1, keepdims=True)
    rstd2 = lax.rsqrt(square2 - mean2 * mean2 + EPS)
    done = (final - fold_rows(mean2)) * fold_rows(rstd2) * own_columns(g2r_ref) + own_columns(b2r_ref)
    s16[0:8, :] = done
    s16[8:16, :] = roll_half(done)
    out_ref[...] = s16[0:seq, 0:HALF].astype(BF16)
    whole(mom_all, n_tp - 1, PH_MOM).wait_send()


def local(
    hidden_in,
    state,
    lower_bound,
    w_forget,
    w_input,
    w_query,
    w_outgate,
    head_gain,
    w_out,
    ln1_gain,
    ln1_bias,
    routes,
    route_weights,
    exp_gate,
    exp_up,
    exp_down,
    sh_gate,
    sh_up,
    sh_down,
    ln2_gain,
    ln2_bias,
):
    n_tp = lax.axis_size("tp")
    n_ep = lax.axis_size("ep")
    n_x = 4
    seq = hidden_in.shape[0]
    width = w_forget.shape[0]
    per_class = n_ep // CLASSES
    rows_j = 2 * per_class
    operands = (
        hidden_in,
        routes.T,
        route_weights.T,
        w_forget,
        w_input,
        w_query,
        w_outgate,
        lower_bound,
        head_gain.reshape(1, LANES),
        state.reshape(seq, LANES, LANES),
        w_out,
        ln1_gain.reshape(1, width),
        ln1_bias.reshape(1, width),
        sh_gate.T,
        sh_up.T,
        sh_down,
        ln1_gain.reshape(width // LANES, LANES),
        ln1_bias.reshape(width // LANES, LANES),
        exp_gate,
        exp_down,
        ln2_gain.reshape(width // LANES, LANES),
        ln2_bias.reshape(width // LANES, LANES),
        exp_up,
    )
    held = [pltpu.VMEM(a.shape, a.dtype) for a in operands]
    held[18] = pltpu.VMEM((2, width, 2 * LANES), BF16)
    held[22] = pltpu.VMEM((8, LANES), F32)
    vmem = pl.BlockSpec(memory_space=pltpu.VMEM)
    hbm = pl.BlockSpec(memory_space=pltpu.HBM)
    sem = pltpu.SemaphoreType.DMA
    tile = (8, LANES)
    mixed_out, new_state = pl.pallas_call(
        functools.partial(kernel, n_tp, n_ep, n_x),
        out_shape=(
            jax.ShapeDtypeStruct(hidden_in.shape, BF16),
            jax.ShapeDtypeStruct((seq, LANES, LANES), F32),
        ),
        in_specs=[hbm] * len(operands),
        out_specs=(vmem, hbm),
        scratch_shapes=[
            *held,
            pltpu.VMEM((16, LANES), F32),
            pltpu.VMEM((LANES, LANES), F32),
            pltpu.VMEM(tile, BF16),
            pltpu.VMEM((n_tp, *tile), BF16),
            pltpu.VMEM((n_ep, 1, LANES), F32),
            pltpu.VMEM((n_ep, 1, LANES), F32),
            pltpu.VMEM((n_ep, *tile), F32),
            pltpu.VMEM((n_ep, *tile), F32),
            pltpu.VMEM((CLASSES, 4 * rows_j, 8 * per_class), BF16),
            pltpu.VMEM((n_tp, *tile), BF16),
            pltpu.VMEM((n_tp, *tile), BF16),
            pltpu.VMEM(tile, BF16),
            pltpu.VMEM((n_tp, *tile), BF16),
            pltpu.VMEM((n_ep, *tile), BF16),
            pltpu.VMEM((CLASSES, rows_j, LANES), BF16),
            pltpu.VMEM((CLASSES, n_tp, rows_j, LANES), BF16),
            pltpu.VMEM((2 * rows_j, width), F32),
            pltpu.VMEM((2 * rows_j, width), BF16),
            pltpu.VMEM((n_tp, *tile), BF16),
            pltpu.VMEM((n_tp, *tile), BF16),
            pltpu.VMEM((CLASSES, n_tp, rows_j, LANES), BF16),
            pltpu.VMEM((CLASSES, n_tp, rows_j, LANES), BF16),
            pltpu.VMEM((n_ep, *tile), BF16),
            pltpu.VMEM((n_ep, *tile), BF16),
            pltpu.VMEM((1, LANES), F32),
            pltpu.VMEM((n_tp, 1, LANES), F32),
            sem((24,)),
            sem((N_PH,)),
            sem((N_PH,)),
        ],
        compiler_params=pltpu.CompilerParams(collective_id=0, has_side_effects=True),
        name="decode_step",
    )(*operands)
    return (mixed_out, new_state.reshape(state.shape))


def solution(mesh):
    placed = (
        P("ep", "tp"),
        P("ep", "tp", None, None),
        P("tp", None),
        P(None, "tp"),
        P(None, "tp"),
        P(None, "tp"),
        P(None, "tp"),
        P(),
        P("tp", None),
        P(),
        P(),
        P("ep", None),
        P("ep", None),
        P("ep", None, "tp"),
        P("ep", None, "tp"),
        P("ep", "tp", None),
        P(None, "tp"),
        P(None, "tp"),
        P("tp", None),
        P(),
        P(),
    )
    return jax.shard_map(
        local,
        mesh=mesh,
        in_specs=placed,
        out_specs=(P("ep", "tp"), P("ep", "tp", None, None)),
        check_vma=False,
    )
```

```python
import functools

import jax
import jax.numpy as jnp
from jax import lax
from jax.experimental import pallas as pl
from jax.experimental.pallas import tpu as pltpu
from jax.sharding import PartitionSpec as P

EPS = 1e-05
ALPHA = 2.0**0.25
MESH = pl.DeviceIdType.MESH
F32 = jnp.float32
BF16 = jnp.bfloat16
LANES = 128
HALF = 64

PH_HID, PH_MIX, PH_RS, PH_ROWS, PH_RET, PH_MOM, PH_SH, PH_EP, PH_PICK, PH_OUT = 0, 1, 2, 3, 4, 5, 6, 7, 10, 13
N_PH = 16
CLASSES = 3


def roll_half(x):
    return pltpu.roll(x, HALF, x.ndim - 1)


def low_lanes(shape):
    return lax.broadcasted_iota(jnp.int32, shape, len(shape) - 1) < HALF


def spread(k):
    return lax.div(k + 1, 2) * (2 * lax.rem(k, 2) - 1)


def wrap(i, n):
    return jnp.where(i >= n, i - n, i)


def finish(mixed_ref, state_ref, mixed_hbm, state_hbm, sems):
    copies = (
        pltpu.make_async_copy(state_ref, state_hbm, sems.at[0]),
        pltpu.make_async_copy(mixed_ref, mixed_hbm, sems.at[1]),
    )
    for copy in copies:
        copy.start()
    for copy in copies:
        copy.wait()


def kernel(n_tp, n_ep, n_x, *refs):
    hbm, refs = refs[:23], refs[23:]
    (out_ref, ns_ref), refs = refs[:2], refs[2:]
    vm, refs = refs[:23], refs[23:]
    (
        s16,
        s128,
        hid_t,
        hid_all,
        mix_s,
        mix_r,
        mix_low,
        mix_high,
        choose,
        rs_s,
        rs_r,
        row_t,
        row_all,
        ep_all,
        pick_t,
        pick_all,
        xrow,
        xnorm,
        sh_s,
        sh_r,
        out_s,
        out_r,
        ret_s,
        ret_r,
        mom_t,
        mom_all,
        lsem,
        ssem,
        rsem,
    ) = refs
    (
        hid_ref,
        routes_ref,
        rw_ref,
        wf,
        wi,
        wq,
        wg,
        lb_ref,
        hg_ref,
        state,
        wout,
        g1_ref,
        b1_ref,
        shg_ref,
        shu_ref,
        shd_ref,
        g1r_ref,
        b1r_ref,
        egu,
        ed,
        g2r_ref,
        b2r_ref,
    ) = vm[:22]
    egu_extra = hbm[22]

    g = lax.axis_index("ep")
    t = lax.axis_index("tp")
    core = lax.rem(g, 2)
    z = g // 2
    n_z = n_ep // 2
    n_y = n_tp // n_x
    y = t // n_x
    x = lax.rem(t, n_x)
    pairs = n_tp // 2
    seq = hid_ref.shape[0]
    width = n_tp * HALF
    per_class = n_ep // CLASSES
    rows_j = 2 * per_class

    barrier = pltpu.get_barrier_semaphore()

    def ep_peer(i):
        half = lax.div(i, 2)
        k = (n_z - 1) - half
        odd = i - 2 * half
        to_core = jnp.where(odd == 0, 1 - core, core)
        chip = z - spread(k)
        chip = wrap(jnp.where(chip < 0, chip + n_z, chip), n_z)
        return k, 2 * chip + to_core

    def greet_tp(i, c):
        pl.semaphore_signal(barrier, inc=1, device_id={"tp": wrap(t + i, n_tp)}, device_id_type=MESH)
        return c

    def greet_ep(i, c):
        pl.semaphore_signal(barrier, inc=1, device_id={"ep": wrap(g + i, n_ep)}, device_id_type=MESH)
        return c

    pltpu.make_async_copy(hbm[0], hid_ref, lsem.at[0]).start()
    lax.fori_loop(1, n_ep, greet_ep, 0)
    lax.fori_loop(1, n_tp, greet_tp, 0)

    columns = [wrap(x + dx, n_x) for dx in range(n_x)]
    by_distance = [n_x // 2] + [d for k in range(1, n_x) for d in [n_x // 2 + ((k + 1) // 2) * (2 * (k % 2) - 1)] if d % n_x] + [0]

    def tp_each(send):
        def body(k, c):
            base = n_x * wrap(y + n_y // 2 + spread(k), n_y)
            for dx in by_distance:
                send(base + columns[dx])
            return c

        lax.fori_loop(0, n_y - 1, body, 0)
        for dx in by_distance[:-1]:
            send(n_x * y + columns[dx])

    loads = []
    for i in range(22):
        if i == 18:
            loads.append(
                [
                    pltpu.make_async_copy(hbm[i], egu.at[:, :, 0:LANES], lsem.at[i]),
                    pltpu.make_async_copy(egu_extra, egu.at[:, :, LANES : 2 * LANES], lsem.at[22]),
                ]
            )
        else:
            loads.append([pltpu.make_async_copy(hbm[i], vm[i], lsem.at[i])])
    for group in loads[1:]:
        for load in group:
            load.start()

    def ready(*which):
        for i in which:
            for load in loads[i]:
                load.wait()

    def remote(src, dst, ph, device):
        return pltpu.make_async_remote_copy(
            src_ref=src,
            dst_ref=dst,
            send_sem=ssem.at[ph],
            recv_sem=rsem.at[ph],
            device_id=device,
            device_id_type=MESH,
        )

    def tp_tile(src, dst, ph):
        tp_each(lambda p: remote(src, dst.at[t], ph, {"tp": p}).start())

    def tp_tiles(src, dst, ph):
        tp_each(lambda p: remote(src.at[p], dst.at[t], ph, {"tp": p}).start())

    def whole(buf, count, ph):
        part = buf.at[pl.ds(0, count)]
        return remote(part, part, ph, {"tp": wrap(t + 1, n_tp)})

    low8 = low_lanes((8, LANES))
    s16[...] = jnp.zeros_like(s16)
    ready(0)
    s16[0:seq, 0:HALF] = hid_ref[...].astype(F32)
    hid_own = s16[0:8, :] + roll_half(s16[8:16, :])
    hid_t[...] = hid_own.astype(BF16)
    hid_all[t] = hid_own.astype(BF16)

    pl.semaphore_wait(barrier, n_ep + n_tp - 2)
    tp_tile(hid_t, hid_all, PH_HID)

    ready(1, 2)
    s128[...] = jnp.zeros_like(s128)
    s128[0:4, 0:seq] = routes_ref[...].astype(F32)
    s128[8:12, 0:seq] = rw_ref[...]
    by_row = jnp.transpose(s128[...])[0:16, :]
    lane16 = lax.broadcasted_iota(jnp.int32, (16, LANES), 1)
    row16 = lax.broadcasted_iota(jnp.int32, (16, LANES), 0)
    expert_of = (lane16 // 2).astype(F32)
    place_of = (lane16 % 2).astype(F32)
    named = jnp.zeros((16, LANES), F32)
    weight = jnp.zeros((16, LANES), F32)
    for k in range(4):
        hit = (by_row[:, k : k + 1] == expert_of) & (row16 < seq)
        named = named + jnp.where(hit, 1.0, 0.0)
        weight = weight + jnp.where(hit, by_row[:, 8 + k : 9 + k], 0.0)
    earlier = jnp.where(
        lax.broadcasted_iota(jnp.int32, (16, 16), 1) < lax.broadcasted_iota(jnp.int32, (16, 16), 0), 1.0, 0.0
    ).astype(BF16)
    before = jnp.dot(earlier, named.astype(BF16), preferred_element_type=F32)
    weight = jnp.where(before == place_of, weight, 0.0)
    s128[...] = jnp.zeros_like(s128)
    s128[0:16, :] = weight
    by_code = jnp.transpose(s128[...])
    lane32 = lax.broadcasted_iota(jnp.int32, (32, LANES), 1)
    row32 = lax.broadcasted_iota(jnp.int32, (32, LANES), 0)
    message = jnp.zeros((32, LANES), F32)
    for c in range(4):
        take = jnp.where(lane32 == 4 * row32 + c, 1.0, 0.0)
        part = jnp.dot(take, by_code, precision=lax.Precision.HIGHEST, preferred_element_type=F32)
        message = message + (part if c == 0 else pltpu.roll(part, 16 * c, 1))
    for e in range(n_ep):
        mix_s[e] = message[e : e + 1, :]
    mix_r[core] = mix_s[g]

    def mix_send(i, c):
        k, e = ep_peer(i)
        remote(mix_s.at[e], mix_r.at[2 * k + core], PH_MIX, {"ep": e}).start()
        return c

    lax.fori_loop(0, n_ep - 1, mix_send, 0)

    def full_rows(buf):
        left, right = [], []
        for p in range(pairs):
            a = buf[2 * p].astype(F32)
            b = buf[2 * p + 1].astype(F32)
            left.append(jnp.where(low8, a, roll_half(b)))
            right.append(jnp.where(low8, roll_half(a), b))
        return jnp.concatenate([jnp.concatenate(left, 1), jnp.concatenate(right, 1)], 0)

    whole(hid_all, n_tp - 1, PH_HID).wait_recv()
    rows = full_rows(hid_all).astype(BF16)

    def project(i):
        ready(i)
        return jnp.dot(rows, vm[i][...], preferred_element_type=F32).astype(BF16).astype(F32)

    forget_pre = project(3)
    values = project(4)
    queries = project(5)
    queries = queries * jax.nn.sigmoid(queries)
    gate = project(6)
    gate = gate * jax.nn.sigmoid(gate)
    ready(7, 8)
    lower = lb_ref[...]
    forget = lower + (1.0 - lower) * jax.nn.sigmoid(forget_pre)
    key = (1.0 - lower) * jax.nn.sigmoid(-forget_pre)

    s128[0:16, :] = queries * forget
    by_channel = jnp.transpose(s128[...])
    ready(9)
    for b in range(seq):
        s16[b : b + 1, :] = jnp.sum(by_channel[:, b : b + 1] * state[b], axis=0, keepdims=True)
    s16[seq:16, :] = jnp.zeros((16 - seq, LANES), F32)
    readout = s16[...] + jnp.sum(queries * key, axis=1, keepdims=True) * values
    mean_sq = jnp.mean(readout * readout, axis=1, keepdims=True)
    mixed = (readout * lax.rsqrt(mean_sq + EPS) * hg_ref[...] * gate).astype(BF16)

    def fold_out(top, bottom, p, buf):
        low = low_lanes(top.shape)
        buf[2 * p] = jnp.where(low, top, roll_half(bottom)).astype(BF16)
        buf[2 * p + 1] = jnp.where(low, roll_half(top), bottom).astype(BF16)

    ready(10)
    branch = jnp.dot(mixed, wout[...], preferred_element_type=F32)
    for p in range(pairs):
        block = branch[:, p * LANES : (p + 1) * LANES]
        fold_out(block[0:8], block[8:16], p, rs_s)
    rs_r[t] = rs_s[t]
    tp_tiles(rs_s, rs_r, PH_RS)

    s128[0:16, :] = forget
    forget_col = jnp.transpose(s128[...])
    s128[0:16, :] = key
    key_col = jnp.transpose(s128[...])
    for b in range(seq):
        ns_ref[b] = forget_col[:, b : b + 1] * state[b] + key_col[:, b : b + 1] * values[b : b + 1, :]

    whole(mix_r, n_ep - 1, PH_MIX).wait_recv()
    lane8 = lax.broadcasted_iota(jnp.int32, (8, LANES), 1)
    row8 = lax.broadcasted_iota(jnp.int32, (8, LANES), 0)
    mask_low = (lane8 < HALF) & (lane8 % 16 == row8)
    mask_high = (lane8 < HALF) & (lane8 % 16 == row8 + 8)
    every = [jnp.broadcast_to(mix_r[r], (8, LANES)) for r in range(n_ep)]
    from_lane = lax.broadcasted_iota(jnp.int32, (LANES, LANES), 0)
    to_lane = lax.broadcasted_iota(jnp.int32, (LANES, LANES), 1)
    place = jnp.where(
        (from_lane < HALF) & (to_lane == (from_lane // 32) * rows_j + (from_lane // 16) % 2), 1.0, 0.0
    )
    for mask, keep in ((mask_low, mix_low), (mask_high, mix_high)):
        stacked = jnp.concatenate([jnp.where(mask, row, 0.0) for row in every], 0)
        placed = jnp.dot(stacked, place, precision=lax.Precision.HIGHEST, preferred_element_type=F32)
        for r in range(n_ep):
            at = 2 * (r % per_class)
            piece = placed[8 * r : 8 * r + 8]
            keep[r] = piece if at == 0 else pltpu.roll(piece, at, 1)
    for c in range(CLASSES):
        part = slice(c * per_class, (c + 1) * per_class)
        low_c = jnp.where(mix_low[part].reshape(8 * per_class, LANES) != 0.0, 1.0, 0.0)
        high_c = jnp.where(mix_high[part].reshape(8 * per_class, LANES) != 0.0, 1.0, 0.0)
        s128[0 : 8 * per_class, :] = low_c + pltpu.roll(high_c, 2 * rows_j, 1)
        choose[c] = jnp.transpose(s128[...])[0 : 4 * rows_j, 0 : 8 * per_class].astype(BF16)

    whole(rs_r, n_tp - 1, PH_RS).wait_recv()
    own = ALPHA * hid_own + jnp.sum(rs_r[...].astype(F32), axis=0)
    row_t[...] = own.astype(BF16)
    row_all[t] = own.astype(BF16)
    ep_all[core] = own.astype(BF16)

    def ep_send(i, c):
        k, e = ep_peer(i)
        remote(row_t, ep_all.at[2 * k + core], PH_EP + lax.div(2 * k, per_class), {"ep": e}).start()
        return c

    lax.fori_loop(0, n_ep - 1, ep_send, 0)
    tp_tile(row_t, row_all, PH_ROWS)

    low_j = low_lanes((rows_j, LANES))
    one, two = slice(0, rows_j), slice(rows_j, 2 * rows_j)
    for c in range(CLASSES):
        whole(ep_all, per_class - 1 if c == 0 else per_class, PH_EP + c).wait_recv()
        tiles = ep_all[c * per_class : (c + 1) * per_class].astype(F32).reshape(8 * per_class, LANES).astype(BF16)
        got = jnp.dot(choose[c], tiles, preferred_element_type=F32)
        got_low, got_high = got[0 : 2 * rows_j], got[2 * rows_j : 4 * rows_j]
        picked = jnp.where(
            low_j,
            got_low[one] + roll_half(got_high[one]),
            roll_half(got_low[two]) + got_high[two],
        ).astype(BF16)
        pick_t[c] = picked
        pick_all[c, t] = picked
        tp_tile(pick_t.at[c], pick_all.at[c], PH_PICK + c)

    ready(11, 12, 13, 14, 15, 16, 17)
    whole(row_all, n_tp - 1, PH_ROWS).wait_recv()
    full = full_rows(row_all)
    mean1 = jnp.mean(full, axis=1, keepdims=True)
    centred = full - mean1
    rstd1 = lax.rsqrt(jnp.mean(centred * centred, axis=1, keepdims=True) + EPS)
    normed = (centred * rstd1 * g1_ref[...] + b1_ref[...]).astype(BF16)
    over_cols = (((1,), (1,)), ((), ()))
    sh_gate = lax.dot_general(normed, shg_ref[...], over_cols, preferred_element_type=F32)
    sh_up = lax.dot_general(normed, shu_ref[...], over_cols, preferred_element_type=F32)
    sh_hidden = (sh_gate * jax.nn.sigmoid(sh_gate) * sh_up).astype(BF16)
    shared = jnp.dot(sh_hidden, shd_ref[...], preferred_element_type=F32)
    for p in range(pairs):
        block = shared[:, p * LANES : (p + 1) * LANES]
        fold_out(block[0:8], block[8:16], p, sh_s)

    def own_columns(ref):
        row = jnp.broadcast_to(ref[pl.ds(t // 2, 1), :], (8, LANES))
        swapped = roll_half(row)
        even = lax.rem(t, 2) == 0
        return jnp.where(low8, jnp.where(even, row, swapped), jnp.where(even, swapped, row))

    def fold_rows(col):
        return jnp.where(low8, col[0:8], col[8:16])

    own_normed = ((own - fold_rows(mean1)) * fold_rows(rstd1) * own_columns(g1r_ref) + own_columns(b1r_ref)).astype(
        BF16
    ).astype(F32)

    ready(18, 19)
    for c in range(CLASSES):
        whole(pick_all.at[c], n_tp - 1, PH_PICK + c).wait_recv()
        sums = [jnp.zeros((rows_j, LANES), F32), jnp.zeros((rows_j, LANES), F32)]
        for p in range(pairs):
            a = pick_all[c, 2 * p].astype(F32)
            b = pick_all[c, 2 * p + 1].astype(F32)
            cols = slice(p * LANES, (p + 1) * LANES)
            x0 = jnp.where(low_j, a, roll_half(b))
            x1 = jnp.where(low_j, roll_half(a), b)
            xrow[one, cols] = x0
            xrow[two, cols] = x1
            sums = [sums[0] + x0, sums[1] + x1]
        hidden = []
        for j, at in enumerate((one, two)):
            mean = jnp.sum(sums[j], axis=1, keepdims=True) / width
            total = jnp.zeros((rows_j, LANES), F32)
            for p in range(pairs):
                d = xrow[at, p * LANES : (p + 1) * LANES] - mean
                total = total + d * d
            rstd = lax.rsqrt(jnp.sum(total, axis=1, keepdims=True) / width + EPS)
            for p in range(pairs):
                cols = slice(p * LANES, (p + 1) * LANES)
                xnorm[at, cols] = ((xrow[at, cols] - mean) * rstd * g1_ref[:, cols] + b1_ref[:, cols]).astype(BF16)
            both = jnp.dot(xnorm[at, :], egu[j], preferred_element_type=F32)
            gate_j, up_j = both[:, 0:LANES], both[:, LANES : 2 * LANES]
            hidden.append((gate_j * jax.nn.sigmoid(gate_j) * up_j).astype(BF16))
        step = min(256, width)
        for n in range(width // step):
            cols = slice(n * step, (n + 1) * step)
            y0 = jnp.dot(hidden[0], ed[0, :, cols], preferred_element_type=F32)
            y1 = jnp.dot(hidden[1], ed[1, :, cols], preferred_element_type=F32)
            for q in range(step // LANES):
                sub = slice(q * LANES, (q + 1) * LANES)
                fold_out(y0[:, sub], y1[:, sub], n * (step // LANES) + q, out_s.at[c])
        out_r[c, t] = out_s[c, t]
        tp_tiles(out_s.at[c], out_r.at[c], PH_OUT + c)
        if c == 0:
            sh_r[t] = sh_s[t]
            tp_tiles(sh_s, sh_r, PH_SH)

    for c in range(CLASSES):
        whole(out_r.at[c], n_tp - 1, PH_OUT + c).wait_recv()
        slots = jnp.sum(out_r[c].astype(F32), axis=0)
        turned = roll_half(slots)
        both = jnp.concatenate([jnp.where(low_j, slots, turned), jnp.where(low_j, turned, slots)], 0)
        part = slice(c * per_class, (c + 1) * per_class)
        low_c = mix_low[part].reshape(8 * per_class, LANES)[:, 0 : 2 * rows_j]
        high_c = mix_high[part].reshape(8 * per_class, LANES)[:, 0 : 2 * rows_j]
        back_low = jnp.dot(low_c, both, precision=lax.Precision.HIGHEST, preferred_element_type=F32)
        back_high = jnp.dot(high_c, both, precision=lax.Precision.HIGHEST, preferred_element_type=F32)
        back = jnp.where(low_lanes((8 * per_class, LANES)), back_low, back_high)
        ret_s[part] = back.reshape(per_class, 8, LANES).astype(BF16)
        if c == 0:
            ret_r[g] = ret_s[core]

        def ret_send(i, carry, c=c):
            r = c * per_class + i
            half = lax.div(r, 2)
            chip = z + spread(half)
            chip = wrap(jnp.where(chip < 0, chip + n_z, chip), n_z)
            e = 2 * chip + r - 2 * half

            @pl.when(e != g)
            def _():
                remote(ret_s.at[r], ret_r.at[g], PH_RET, {"ep": e}).start()

            return carry

        lax.fori_loop(0, per_class, ret_send, 0)

    ready(20, 21)
    whole(sh_r, n_tp - 1, PH_SH).wait_recv()
    final = ALPHA * own_normed + jnp.sum(sh_r[...].astype(F32), axis=0)
    whole(ret_r, n_ep - 1, PH_RET).wait_recv()
    final = final + jnp.sum(ret_r[...].astype(F32), axis=0)

    mine = jnp.concatenate([jnp.where(low8, final, 0.0), jnp.where(low8, roll_half(final), 0.0)], 0)
    part = jnp.where(lane16 == row16, jnp.sum(mine, axis=1, keepdims=True), 0.0) + jnp.where(
        lane16 == row16 + 16, jnp.sum(mine * mine, axis=1, keepdims=True), 0.0
    )
    part = jnp.sum(part, axis=0, keepdims=True)
    mom_t[...] = part
    mom_all[t] = part
    tp_tile(mom_t, mom_all, PH_MOM)
    for buf, count, ph in (
        (hid_all, n_tp - 1, PH_HID),
        (mix_r, n_ep - 1, PH_MIX),
        (rs_r, n_tp - 1, PH_RS),
        (row_all, n_tp - 1, PH_ROWS),
        (sh_r, n_tp - 1, PH_SH),
        (ret_r, n_ep - 1, PH_RET),
    ):
        whole(buf, count, ph).wait_send()
    for c in range(CLASSES):
        whole(ep_all, per_class - 1 if c == 0 else per_class, PH_EP + c).wait_send()
        whole(pick_all.at[c], n_tp - 1, PH_PICK + c).wait_send()
        whole(out_r.at[c], n_tp - 1, PH_OUT + c).wait_send()
    whole(mom_all, n_tp - 1, PH_MOM).wait_recv()
    moments = jnp.broadcast_to(jnp.sum(mom_all[...], axis=0) / width, (16, LANES))
    mean2 = jnp.sum(jnp.where(lane16 == row16, moments, 0.0), axis=1, keepdims=True)
    square2 = jnp.sum(jnp.where(lane16 == row16 + 16, moments, 0.0), axis=1, keepdims=True)
    rstd2 = lax.rsqrt(square2 - mean2 * mean2 + EPS)
    done = (final - fold_rows(mean2)) * fold_rows(rstd2) * own_columns(g2r_ref) + own_columns(b2r_ref)
    s16[0:8, :] = done
    s16[8:16, :] = roll_half(done)
    out_ref[...] = s16[0:seq, 0:HALF].astype(BF16)
    whole(mom_all, n_tp - 1, PH_MOM).wait_send()


def local(
    hidden_in,
    state,
    lower_bound,
    w_forget,
    w_input,
    w_query,
    w_outgate,
    head_gain,
    w_out,
    ln1_gain,
    ln1_bias,
    routes,
    route_weights,
    exp_gate,
    exp_up,
    exp_down,
    sh_gate,
    sh_up,
    sh_down,
    ln2_gain,
    ln2_bias,
):
    n_tp = lax.axis_size("tp")
    n_ep = lax.axis_size("ep")
    n_x = 4
    seq = hidden_in.shape[0]
    width = w_forget.shape[0]
    per_class = n_ep // CLASSES
    rows_j = 2 * per_class
    operands = (
        hidden_in,
        routes.T,
        route_weights.T,
        w_forget,
        w_input,
        w_query,
        w_outgate,
        lower_bound,
        head_gain.reshape(1, LANES),
        state.reshape(seq, LANES, LANES),
        w_out,
        ln1_gain.reshape(1, width),
        ln1_bias.reshape(1, width),
        sh_gate.T,
        sh_up.T,
        sh_down,
        ln1_gain.reshape(width // LANES, LANES),
        ln1_bias.reshape(width // LANES, LANES),
        exp_gate,
        exp_down,
        ln2_gain.reshape(width // LANES, LANES),
        ln2_bias.reshape(width // LANES, LANES),
        exp_up,
    )
    held = [pltpu.VMEM(a.shape, a.dtype) for a in operands]
    held[18] = pltpu.VMEM((2, width, 2 * LANES), BF16)
    held[22] = pltpu.VMEM((8, LANES), F32)
    vmem = pl.BlockSpec(memory_space=pltpu.VMEM)
    hbm = pl.BlockSpec(memory_space=pltpu.HBM)
    sem = pltpu.SemaphoreType.DMA
    tile = (8, LANES)
    mixed_out, new_state = pl.pallas_call(
        functools.partial(kernel, n_tp, n_ep, n_x),
        out_shape=(pltpu.VMEM(hidden_in.shape, BF16), pltpu.VMEM((seq, LANES, LANES), F32)),
        in_specs=[hbm] * len(operands),
        out_specs=(vmem, vmem),
        scratch_shapes=[
            *held,
            pltpu.VMEM((16, LANES), F32),
            pltpu.VMEM((LANES, LANES), F32),
            pltpu.VMEM(tile, BF16),
            pltpu.VMEM((n_tp, *tile), BF16),
            pltpu.VMEM((n_ep, 1, LANES), F32),
            pltpu.VMEM((n_ep, 1, LANES), F32),
            pltpu.VMEM((n_ep, *tile), F32),
            pltpu.VMEM((n_ep, *tile), F32),
            pltpu.VMEM((CLASSES, 4 * rows_j, 8 * per_class), BF16),
            pltpu.VMEM((n_tp, *tile), BF16),
            pltpu.VMEM((n_tp, *tile), BF16),
            pltpu.VMEM(tile, BF16),
            pltpu.VMEM((n_tp, *tile), BF16),
            pltpu.VMEM((n_ep, *tile), BF16),
            pltpu.VMEM((CLASSES, rows_j, LANES), BF16),
            pltpu.VMEM((CLASSES, n_tp, rows_j, LANES), BF16),
            pltpu.VMEM((2 * rows_j, width), F32),
            pltpu.VMEM((2 * rows_j, width), BF16),
            pltpu.VMEM((n_tp, *tile), BF16),
            pltpu.VMEM((n_tp, *tile), BF16),
            pltpu.VMEM((CLASSES, n_tp, rows_j, LANES), BF16),
            pltpu.VMEM((CLASSES, n_tp, rows_j, LANES), BF16),
            pltpu.VMEM((n_ep, *tile), BF16),
            pltpu.VMEM((n_ep, *tile), BF16),
            pltpu.VMEM((1, LANES), F32),
            pltpu.VMEM((n_tp, 1, LANES), F32),
            sem((24,)),
            sem((N_PH,)),
            sem((N_PH,)),
        ],
        compiler_params=pltpu.CompilerParams(collective_id=0, has_side_effects=True),
        name="decode_step",
    )(*operands)
    mixed_out, new_state = pl.pallas_call(
        finish,
        out_shape=(
            jax.ShapeDtypeStruct(hidden_in.shape, BF16),
            jax.ShapeDtypeStruct((seq, LANES, LANES), F32),
        ),
        in_specs=[vmem] * 2,
        out_specs=(hbm, hbm),
        scratch_shapes=[sem((2,))],
        name="write_out",
    )(
        pltpu.with_memory_space_constraint(mixed_out, pltpu.VMEM),
        pltpu.with_memory_space_constraint(new_state, pltpu.VMEM),
    )
    return (mixed_out, new_state.reshape(state.shape))


def solution(mesh):
    placed = (
        P("ep", "tp"),
        P("ep", "tp", None, None),
        P("tp", None),
        P(None, "tp"),
        P(None, "tp"),
        P(None, "tp"),
        P(None, "tp"),
        P(),
        P("tp", None),
        P(),
        P(),
        P("ep", None),
        P("ep", None),
        P("ep", None, "tp"),
        P("ep", None, "tp"),
        P("ep", "tp", None),
        P(None, "tp"),
        P(None, "tp"),
        P("tp", None),
        P(),
        P(),
    )
    return jax.shard_map(
        local,
        mesh=mesh,
        in_specs=placed,
        out_specs=(P("ep", "tp"), P("ep", "tp", None, None)),
        check_vma=False,
    )
```

```python
import functools

import jax
import jax.numpy as jnp
from jax import lax
from jax.experimental import pallas as pl
from jax.experimental.pallas import tpu as pltpu
from jax.sharding import PartitionSpec as P

EPS = 1e-05
ALPHA = 2.0**0.25
MESH = pl.DeviceIdType.MESH
F32 = jnp.float32
BF16 = jnp.bfloat16
LANES = 128
HALF = 64

PH_HID, PH_MIX, PH_RS, PH_ROWS, PH_RET, PH_MOM, PH_SH, PH_EP, PH_PICK, PH_OUT = 0, 1, 2, 3, 4, 5, 6, 7, 10, 13
N_PH = 16
CLASSES = 3


def roll_half(x):
    return pltpu.roll(x, HALF, x.ndim - 1)


def low_lanes(shape):
    return lax.broadcasted_iota(jnp.int32, shape, len(shape) - 1) < HALF


def spread(k):
    return lax.div(k + 1, 2) * (2 * lax.rem(k, 2) - 1)


def spread_fixed(k):
    return ((k + 1) // 2) * (2 * (k % 2) - 1)


def wrap(i, n):
    return jnp.where(i >= n, i - n, i)


def finish(mixed_ref, state_ref, mixed_hbm, state_hbm, sems):
    copies = (
        pltpu.make_async_copy(state_ref, state_hbm, sems.at[0]),
        pltpu.make_async_copy(mixed_ref, mixed_hbm, sems.at[1]),
    )
    for copy in copies:
        copy.start()
    for copy in copies:
        copy.wait()


def kernel(n_tp, n_ep, n_x, *refs):
    hbm, refs = refs[:23], refs[23:]
    (out_ref, ns_ref), refs = refs[:2], refs[2:]
    vm, refs = refs[:23], refs[23:]
    (
        s16,
        s128,
        hid_t,
        hid_all,
        mix_s,
        mix_r,
        mix_low,
        mix_high,
        choose,
        rs_s,
        rs_r,
        row_t,
        row_all,
        ep_all,
        pick_t,
        pick_all,
        xrow,
        xnorm,
        sh_s,
        sh_r,
        out_s,
        out_r,
        ret_s,
        ret_r,
        mom_t,
        mom_all,
        lsem,
        ssem,
        rsem,
    ) = refs
    (
        hid_ref,
        routes_ref,
        rw_ref,
        wf,
        wi,
        wq,
        wg,
        lb_ref,
        hg_ref,
        state,
        wout,
        g1_ref,
        b1_ref,
        shg_ref,
        shu_ref,
        shd_ref,
        g1r_ref,
        b1r_ref,
        egu,
        ed,
        g2r_ref,
        b2r_ref,
    ) = vm[:22]
    egu_extra = hbm[22]

    g = lax.axis_index("ep")
    t = lax.axis_index("tp")
    core = lax.rem(g, 2)
    z = g // 2
    n_z = n_ep // 2
    n_y = n_tp // n_x
    y = t // n_x
    x = lax.rem(t, n_x)
    pairs = n_tp // 2
    seq = hid_ref.shape[0]
    width = n_tp * HALF
    per_class = n_ep // CLASSES
    rows_j = 2 * per_class

    barrier = pltpu.get_barrier_semaphore()

    chips = [wrap(z + (spread_fixed(k) + n_z) % n_z, n_z) for k in range(n_z)]

    def chip_behind(k):
        if 2 * spread_fixed(k) == n_z:
            return chips[k]
        return chips[k + 1 if k % 2 else k - 1]

    def ep_each(send):
        send(0, 2 * z + 1 - core)
        for k in range(1, n_z):
            for to_core in range(2):
                send(k, 2 * chip_behind(k) + to_core)

    def greet_tp(i, c):
        pl.semaphore_signal(barrier, inc=1, device_id={"tp": wrap(t + i, n_tp)}, device_id_type=MESH)
        return c

    pltpu.make_async_copy(hbm[0], hid_ref, lsem.at[0]).start()
    ep_each(
        lambda k, e: pl.semaphore_signal(barrier, inc=1, device_id={"ep": e}, device_id_type=MESH)
    )
    lax.fori_loop(1, n_tp, greet_tp, 0)

    columns = [wrap(x + dx, n_x) for dx in range(n_x)]
    by_distance = [n_x // 2] + [d for k in range(1, n_x) for d in [n_x // 2 + ((k + 1) // 2) * (2 * (k % 2) - 1)] if d % n_x] + [0]

    def tp_each(send):
        def body(k, c):
            base = n_x * wrap(y + n_y // 2 + spread(k), n_y)
            for dx in by_distance:
                send(base + columns[dx])
            return c

        lax.fori_loop(0, n_y - 1, body, 0)
        for dx in by_distance[:-1]:
            send(n_x * y + columns[dx])

    loads = []
    for i in range(22):
        if i == 18:
            loads.append(
                [
                    pltpu.make_async_copy(hbm[i], egu.at[:, :, 0:LANES], lsem.at[i]),
                    pltpu.make_async_copy(egu_extra, egu.at[:, :, LANES : 2 * LANES], lsem.at[22]),
                ]
            )
        else:
            loads.append([pltpu.make_async_copy(hbm[i], vm[i], lsem.at[i])])
    for group in loads[1:]:
        for load in group:
            load.start()

    def ready(*which):
        for i in which:
            for load in loads[i]:
                load.wait()

    def remote(src, dst, ph, device):
        return pltpu.make_async_remote_copy(
            src_ref=src,
            dst_ref=dst,
            send_sem=ssem.at[ph],
            recv_sem=rsem.at[ph],
            device_id=device,
            device_id_type=MESH,
        )

    def tp_tile(src, dst, ph):
        tp_each(lambda p: remote(src, dst.at[t], ph, {"tp": p}).start())

    def tp_tiles(src, dst, ph):
        tp_each(lambda p: remote(src.at[p], dst.at[t], ph, {"tp": p}).start())

    def whole(buf, count, ph):
        part = buf.at[pl.ds(0, count)]
        return remote(part, part, ph, {"tp": wrap(t + 1, n_tp)})

    low8 = low_lanes((8, LANES))
    s16[...] = jnp.zeros_like(s16)
    ready(0)
    s16[0:seq, 0:HALF] = hid_ref[...].astype(F32)
    hid_own = s16[0:8, :] + roll_half(s16[8:16, :])
    hid_t[...] = hid_own.astype(BF16)
    hid_all[t] = hid_own.astype(BF16)

    pl.semaphore_wait(barrier, n_ep + n_tp - 2)
    tp_tile(hid_t, hid_all, PH_HID)

    ready(1, 2)
    s128[...] = jnp.zeros_like(s128)
    s128[0:4, 0:seq] = routes_ref[...].astype(F32)
    s128[8:12, 0:seq] = rw_ref[...]
    by_row = jnp.transpose(s128[...])[0:16, :]
    lane16 = lax.broadcasted_iota(jnp.int32, (16, LANES), 1)
    row16 = lax.broadcasted_iota(jnp.int32, (16, LANES), 0)
    expert_of = (lane16 // 2).astype(F32)
    place_of = (lane16 % 2).astype(F32)
    named = jnp.zeros((16, LANES), F32)
    weight = jnp.zeros((16, LANES), F32)
    for k in range(4):
        hit = (by_row[:, k : k + 1] == expert_of) & (row16 < seq)
        named = named + jnp.where(hit, 1.0, 0.0)
        weight = weight + jnp.where(hit, by_row[:, 8 + k : 9 + k], 0.0)
    earlier = jnp.where(
        lax.broadcasted_iota(jnp.int32, (16, 16), 1) < lax.broadcasted_iota(jnp.int32, (16, 16), 0), 1.0, 0.0
    ).astype(BF16)
    before = jnp.dot(earlier, named.astype(BF16), preferred_element_type=F32)
    weight = jnp.where(before == place_of, weight, 0.0)
    s128[...] = jnp.zeros_like(s128)
    s128[0:16, :] = weight
    by_code = jnp.transpose(s128[...])
    lane32 = lax.broadcasted_iota(jnp.int32, (32, LANES), 1)
    row32 = lax.broadcasted_iota(jnp.int32, (32, LANES), 0)
    message = jnp.zeros((32, LANES), F32)
    for c in range(4):
        take = jnp.where(lane32 == 4 * row32 + c, 1.0, 0.0)
        part = jnp.dot(take, by_code, precision=lax.Precision.HIGHEST, preferred_element_type=F32)
        message = message + (part if c == 0 else pltpu.roll(part, 16 * c, 1))
    for e in range(n_ep):
        mix_s[e] = message[e : e + 1, :]
    mix_r[core] = mix_s[g]

    ep_each(lambda k, e: remote(mix_s.at[e], mix_r.at[2 * k + core], PH_MIX, {"ep": e}).start())

    def full_rows(buf):
        left, right = [], []
        for p in range(pairs):
            a = buf[2 * p].astype(F32)
            b = buf[2 * p + 1].astype(F32)
            left.append(jnp.where(low8, a, roll_half(b)))
            right.append(jnp.where(low8, roll_half(a), b))
        return jnp.concatenate([jnp.concatenate(left, 1), jnp.concatenate(right, 1)], 0)

    whole(hid_all, n_tp - 1, PH_HID).wait_recv()
    rows = full_rows(hid_all).astype(BF16)

    def project(i):
        ready(i)
        return jnp.dot(rows, vm[i][...], preferred_element_type=F32).astype(BF16).astype(F32)

    forget_pre = project(3)
    values = project(4)
    queries = project(5)
    queries = queries * jax.nn.sigmoid(queries)
    gate = project(6)
    gate = gate * jax.nn.sigmoid(gate)
    ready(7, 8)
    lower = lb_ref[...]
    forget = lower + (1.0 - lower) * jax.nn.sigmoid(forget_pre)
    key = (1.0 - lower) * jax.nn.sigmoid(-forget_pre)

    s128[0:16, :] = queries * forget
    by_channel = jnp.transpose(s128[...])
    ready(9)
    for b in range(seq):
        s16[b : b + 1, :] = jnp.sum(by_channel[:, b : b + 1] * state[b], axis=0, keepdims=True)
    s16[seq:16, :] = jnp.zeros((16 - seq, LANES), F32)
    readout = s16[...] + jnp.sum(queries * key, axis=1, keepdims=True) * values
    mean_sq = jnp.mean(readout * readout, axis=1, keepdims=True)
    mixed = (readout * lax.rsqrt(mean_sq + EPS) * hg_ref[...] * gate).astype(BF16)

    def fold_out(top, bottom, p, buf):
        low = low_lanes(top.shape)
        buf[2 * p] = jnp.where(low, top, roll_half(bottom)).astype(BF16)
        buf[2 * p + 1] = jnp.where(low, roll_half(top), bottom).astype(BF16)

    ready(10)
    branch = jnp.dot(mixed, wout[...], preferred_element_type=F32)
    for p in range(pairs):
        block = branch[:, p * LANES : (p + 1) * LANES]
        fold_out(block[0:8], block[8:16], p, rs_s)
    rs_r[t] = rs_s[t]
    tp_tiles(rs_s, rs_r, PH_RS)

    s128[0:16, :] = forget
    forget_col = jnp.transpose(s128[...])
    s128[0:16, :] = key
    key_col = jnp.transpose(s128[...])
    for b in range(seq):
        ns_ref[b] = forget_col[:, b : b + 1] * state[b] + key_col[:, b : b + 1] * values[b : b + 1, :]

    whole(mix_r, n_ep - 1, PH_MIX).wait_recv()
    lane8 = lax.broadcasted_iota(jnp.int32, (8, LANES), 1)
    row8 = lax.broadcasted_iota(jnp.int32, (8, LANES), 0)
    mask_low = (lane8 < HALF) & (lane8 % 16 == row8)
    mask_high = (lane8 < HALF) & (lane8 % 16 == row8 + 8)
    every = [jnp.broadcast_to(mix_r[r], (8, LANES)) for r in range(n_ep)]
    from_lane = lax.broadcasted_iota(jnp.int32, (LANES, LANES), 0)
    to_lane = lax.broadcasted_iota(jnp.int32, (LANES, LANES), 1)
    place = jnp.where(
        (from_lane < HALF) & (to_lane == (from_lane // 32) * rows_j + (from_lane // 16) % 2), 1.0, 0.0
    )
    for mask, keep in ((mask_low, mix_low), (mask_high, mix_high)):
        stacked = jnp.concatenate([jnp.where(mask, row, 0.0) for row in every], 0)
        placed = jnp.dot(stacked, place, precision=lax.Precision.HIGHEST, preferred_element_type=F32)
        for r in range(n_ep):
            at = 2 * (r % per_class)
            piece = placed[8 * r : 8 * r + 8]
            keep[r] = piece if at == 0 else pltpu.roll(piece, at, 1)
    for c in range(CLASSES):
        part = slice(c * per_class, (c + 1) * per_class)
        low_c = jnp.where(mix_low[part].reshape(8 * per_class, LANES) != 0.0, 1.0, 0.0)
        high_c = jnp.where(mix_high[part].reshape(8 * per_class, LANES) != 0.0, 1.0, 0.0)
        s128[0 : 8 * per_class, :] = low_c + pltpu.roll(high_c, 2 * rows_j, 1)
        choose[c] = jnp.transpose(s128[...])[0 : 4 * rows_j, 0 : 8 * per_class].astype(BF16)

    whole(rs_r, n_tp - 1, PH_RS).wait_recv()
    own = ALPHA * hid_own + jnp.sum(rs_r[...].astype(F32), axis=0)
    row_t[...] = own.astype(BF16)
    row_all[t] = own.astype(BF16)
    ep_all[core] = own.astype(BF16)

    ep_each(
        lambda k, e: remote(row_t, ep_all.at[2 * k + core], PH_EP + (2 * k) // per_class, {"ep": e}).start()
    )

    low_j = low_lanes((rows_j, LANES))
    one, two = slice(0, rows_j), slice(rows_j, 2 * rows_j)
    for c in range(CLASSES):
        whole(ep_all, per_class - 1 if c == 0 else per_class, PH_EP + c).wait_recv()
        tiles = ep_all[c * per_class : (c + 1) * per_class].astype(F32).reshape(8 * per_class, LANES).astype(BF16)
        got = jnp.dot(choose[c], tiles, preferred_element_type=F32)
        got_low, got_high = got[0 : 2 * rows_j], got[2 * rows_j : 4 * rows_j]
        picked = jnp.where(
            low_j,
            got_low[one] + roll_half(got_high[one]),
            roll_half(got_low[two]) + got_high[two],
        ).astype(BF16)
        pick_t[c] = picked
        pick_all[c, t] = picked
        tp_tile(pick_t.at[c], pick_all.at[c], PH_PICK + c)
        if c == 0:
            tp_tile(row_t, row_all, PH_ROWS)

    ready(11, 12, 13, 14, 15, 16, 17)
    whole(row_all, n_tp - 1, PH_ROWS).wait_recv()
    full = full_rows(row_all)
    mean1 = jnp.mean(full, axis=1, keepdims=True)
    centred = full - mean1
    rstd1 = lax.rsqrt(jnp.mean(centred * centred, axis=1, keepdims=True) + EPS)
    normed = (centred * rstd1 * g1_ref[...] + b1_ref[...]).astype(BF16)
    over_cols = (((1,), (1,)), ((), ()))
    sh_gate = lax.dot_general(normed, shg_ref[...], over_cols, preferred_element_type=F32)
    sh_up = lax.dot_general(normed, shu_ref[...], over_cols, preferred_element_type=F32)
    sh_hidden = (sh_gate * jax.nn.sigmoid(sh_gate) * sh_up).astype(BF16)
    shared = jnp.dot(sh_hidden, shd_ref[...], preferred_element_type=F32)
    for p in range(pairs):
        block = shared[:, p * LANES : (p + 1) * LANES]
        fold_out(block[0:8], block[8:16], p, sh_s)

    def own_columns(ref):
        row = jnp.broadcast_to(ref[pl.ds(t // 2, 1), :], (8, LANES))
        swapped = roll_half(row)
        even = lax.rem(t, 2) == 0
        return jnp.where(low8, jnp.where(even, row, swapped), jnp.where(even, swapped, row))

    def fold_rows(col):
        return jnp.where(low8, col[0:8], col[8:16])

    own_normed = ((own - fold_rows(mean1)) * fold_rows(rstd1) * own_columns(g1r_ref) + own_columns(b1r_ref)).astype(
        BF16
    ).astype(F32)

    ready(18, 19)
    for c in range(CLASSES):
        whole(pick_all.at[c], n_tp - 1, PH_PICK + c).wait_recv()
        sums = [jnp.zeros((rows_j, LANES), F32), jnp.zeros((rows_j, LANES), F32)]
        for p in range(pairs):
            a = pick_all[c, 2 * p].astype(F32)
            b = pick_all[c, 2 * p + 1].astype(F32)
            cols = slice(p * LANES, (p + 1) * LANES)
            x0 = jnp.where(low_j, a, roll_half(b))
            x1 = jnp.where(low_j, roll_half(a), b)
            xrow[one, cols] = x0
            xrow[two, cols] = x1
            sums = [sums[0] + x0, sums[1] + x1]
        hidden = []
        for j, at in enumerate((one, two)):
            mean = jnp.sum(sums[j], axis=1, keepdims=True) / width
            total = jnp.zeros((rows_j, LANES), F32)
            for p in range(pairs):
                d = xrow[at, p * LANES : (p + 1) * LANES] - mean
                total = total + d * d
            rstd = lax.rsqrt(jnp.sum(total, axis=1, keepdims=True) / width + EPS)
            for p in range(pairs):
                cols = slice(p * LANES, (p + 1) * LANES)
                xnorm[at, cols] = ((xrow[at, cols] - mean) * rstd * g1_ref[:, cols] + b1_ref[:, cols]).astype(BF16)
            both = jnp.dot(xnorm[at, :], egu[j], preferred_element_type=F32)
            gate_j, up_j = both[:, 0:LANES], both[:, LANES : 2 * LANES]
            hidden.append((gate_j * jax.nn.sigmoid(gate_j) * up_j).astype(BF16))
        step = min(256, width)
        for n in range(width // step):
            cols = slice(n * step, (n + 1) * step)
            y0 = jnp.dot(hidden[0], ed[0, :, cols], preferred_element_type=F32)
            y1 = jnp.dot(hidden[1], ed[1, :, cols], preferred_element_type=F32)
            for q in range(step // LANES):
                sub = slice(q * LANES, (q + 1) * LANES)
                fold_out(y0[:, sub], y1[:, sub], n * (step // LANES) + q, out_s.at[c])
        out_r[c, t] = out_s[c, t]
        tp_tiles(out_s.at[c], out_r.at[c], PH_OUT + c)
        if c == CLASSES - 1:
            sh_r[t] = sh_s[t]
            tp_tiles(sh_s, sh_r, PH_SH)

    for c in range(CLASSES):
        whole(out_r.at[c], n_tp - 1, PH_OUT + c).wait_recv()
        slots = jnp.sum(out_r[c].astype(F32), axis=0)
        turned = roll_half(slots)
        both = jnp.concatenate([jnp.where(low_j, slots, turned), jnp.where(low_j, turned, slots)], 0)
        part = slice(c * per_class, (c + 1) * per_class)
        low_c = mix_low[part].reshape(8 * per_class, LANES)[:, 0 : 2 * rows_j]
        high_c = mix_high[part].reshape(8 * per_class, LANES)[:, 0 : 2 * rows_j]
        back_low = jnp.dot(low_c, both, precision=lax.Precision.HIGHEST, preferred_element_type=F32)
        back_high = jnp.dot(high_c, both, precision=lax.Precision.HIGHEST, preferred_element_type=F32)
        back = jnp.where(low_lanes((8 * per_class, LANES)), back_low, back_high)
        ret_s[part] = back.reshape(per_class, 8, LANES).astype(BF16)
        if c == 0:
            ret_r[g] = ret_s[core]

        def ret_send(r, e):
            remote(ret_s.at[r], ret_r.at[g], PH_RET, {"ep": e}).start()

        for k in range(c * per_class // 2, (c + 1) * per_class // 2):
            if k == 0:
                ret_send(1 - core, 2 * z + 1 - core)
            else:
                for from_core in range(2):
                    ret_send(2 * k + from_core, 2 * chips[k] + from_core)

    ready(20, 21)
    whole(sh_r, n_tp - 1, PH_SH).wait_recv()
    final = ALPHA * own_normed + jnp.sum(sh_r[...].astype(F32), axis=0)
    whole(ret_r, n_ep - 1, PH_RET).wait_recv()
    final = final + jnp.sum(ret_r[...].astype(F32), axis=0)

    mine = jnp.concatenate([jnp.where(low8, final, 0.0), jnp.where(low8, roll_half(final), 0.0)], 0)
    part = jnp.where(lane16 == row16, jnp.sum(mine, axis=1, keepdims=True), 0.0) + jnp.where(
        lane16 == row16 + 16, jnp.sum(mine * mine, axis=1, keepdims=True), 0.0
    )
    part = jnp.sum(part, axis=0, keepdims=True)
    mom_t[...] = part
    mom_all[t] = part
    tp_tile(mom_t, mom_all, PH_MOM)
    for buf, count, ph in (
        (hid_all, n_tp - 1, PH_HID),
        (mix_r, n_ep - 1, PH_MIX),
        (rs_r, n_tp - 1, PH_RS),
        (row_all, n_tp - 1, PH_ROWS),
        (sh_r, n_tp - 1, PH_SH),
        (ret_r, n_ep - 1, PH_RET),
    ):
        whole(buf, count, ph).wait_send()
    for c in range(CLASSES):
        whole(ep_all, per_class - 1 if c == 0 else per_class, PH_EP + c).wait_send()
        whole(pick_all.at[c], n_tp - 1, PH_PICK + c).wait_send()
        whole(out_r.at[c], n_tp - 1, PH_OUT + c).wait_send()
    whole(mom_all, n_tp - 1, PH_MOM).wait_recv()
    moments = jnp.broadcast_to(jnp.sum(mom_all[...], axis=0) / width, (16, LANES))
    mean2 = jnp.sum(jnp.where(lane16 == row16, moments, 0.0), axis=1, keepdims=True)
    square2 = jnp.sum(jnp.where(lane16 == row16 + 16, moments, 0.0), axis=1, keepdims=True)
    rstd2 = lax.rsqrt(square2 - mean2 * mean2 + EPS)
    done = (final - fold_rows(mean2)) * fold_rows(rstd2) * own_columns(g2r_ref) + own_columns(b2r_ref)
    s16[0:8, :] = done
    s16[8:16, :] = roll_half(done)
    out_ref[...] = s16[0:seq, 0:HALF].astype(BF16)
    whole(mom_all, n_tp - 1, PH_MOM).wait_send()


def local(
    hidden_in,
    state,
    lower_bound,
    w_forget,
    w_input,
    w_query,
    w_outgate,
    head_gain,
    w_out,
    ln1_gain,
    ln1_bias,
    routes,
    route_weights,
    exp_gate,
    exp_up,
    exp_down,
    sh_gate,
    sh_up,
    sh_down,
    ln2_gain,
    ln2_bias,
):
    n_tp = lax.axis_size("tp")
    n_ep = lax.axis_size("ep")
    n_x = 4
    seq = hidden_in.shape[0]
    width = w_forget.shape[0]
    per_class = n_ep // CLASSES
    rows_j = 2 * per_class
    operands = (
        hidden_in,
        routes.T,
        route_weights.T,
        w_forget,
        w_input,
        w_query,
        w_outgate,
        lower_bound,
        head_gain.reshape(1, LANES),
        state.reshape(seq, LANES, LANES),
        w_out,
        ln1_gain.reshape(1, width),
        ln1_bias.reshape(1, width),
        sh_gate.T,
        sh_up.T,
        sh_down,
        ln1_gain.reshape(width // LANES, LANES),
        ln1_bias.reshape(width // LANES, LANES),
        exp_gate,
        exp_down,
        ln2_gain.reshape(width // LANES, LANES),
        ln2_bias.reshape(width // LANES, LANES),
        exp_up,
    )
    held = [pltpu.VMEM(a.shape, a.dtype) for a in operands]
    held[18] = pltpu.VMEM((2, width, 2 * LANES), BF16)
    held[22] = pltpu.VMEM((8, LANES), F32)
    vmem = pl.BlockSpec(memory_space=pltpu.VMEM)
    hbm = pl.BlockSpec(memory_space=pltpu.HBM)
    sem = pltpu.SemaphoreType.DMA
    tile = (8, LANES)
    mixed_out, new_state = pl.pallas_call(
        functools.partial(kernel, n_tp, n_ep, n_x),
        out_shape=(pltpu.VMEM(hidden_in.shape, BF16), pltpu.VMEM((seq, LANES, LANES), F32)),
        in_specs=[hbm] * len(operands),
        out_specs=(vmem, vmem),
        scratch_shapes=[
            *held,
            pltpu.VMEM((16, LANES), F32),
            pltpu.VMEM((LANES, LANES), F32),
            pltpu.VMEM(tile, BF16),
            pltpu.VMEM((n_tp, *tile), BF16),
            pltpu.VMEM((n_ep, 1, LANES), F32),
            pltpu.VMEM((n_ep, 1, LANES), F32),
            pltpu.VMEM((n_ep, *tile), F32),
            pltpu.VMEM((n_ep, *tile), F32),
            pltpu.VMEM((CLASSES, 4 * rows_j, 8 * per_class), BF16),
            pltpu.VMEM((n_tp, *tile), BF16),
            pltpu.VMEM((n_tp, *tile), BF16),
            pltpu.VMEM(tile, BF16),
            pltpu.VMEM((n_tp, *tile), BF16),
            pltpu.VMEM((n_ep, *tile), BF16),
            pltpu.VMEM((CLASSES, rows_j, LANES), BF16),
            pltpu.VMEM((CLASSES, n_tp, rows_j, LANES), BF16),
            pltpu.VMEM((2 * rows_j, width), F32),
            pltpu.VMEM((2 * rows_j, width), BF16),
            pltpu.VMEM((n_tp, *tile), BF16),
            pltpu.VMEM((n_tp, *tile), BF16),
            pltpu.VMEM((CLASSES, n_tp, rows_j, LANES), BF16),
            pltpu.VMEM((CLASSES, n_tp, rows_j, LANES), BF16),
            pltpu.VMEM((n_ep, *tile), BF16),
            pltpu.VMEM((n_ep, *tile), BF16),
            pltpu.VMEM((1, LANES), F32),
            pltpu.VMEM((n_tp, 1, LANES), F32),
            sem((24,)),
            sem((N_PH,)),
            sem((N_PH,)),
        ],
        compiler_params=pltpu.CompilerParams(collective_id=0, has_side_effects=True),
        name="decode_step",
    )(*operands)
    mixed_out, new_state = pl.pallas_call(
        finish,
        out_shape=(
            jax.ShapeDtypeStruct(hidden_in.shape, BF16),
            jax.ShapeDtypeStruct((seq, LANES, LANES), F32),
        ),
        in_specs=[vmem] * 2,
        out_specs=(hbm, hbm),
        scratch_shapes=[sem((2,))],
        name="write_out",
    )(
        pltpu.with_memory_space_constraint(mixed_out, pltpu.VMEM),
        pltpu.with_memory_space_constraint(new_state, pltpu.VMEM),
    )
    return (mixed_out, new_state.reshape(state.shape))


def solution(mesh):
    placed = (
        P("ep", "tp"),
        P("ep", "tp", None, None),
        P("tp", None),
        P(None, "tp"),
        P(None, "tp"),
        P(None, "tp"),
        P(None, "tp"),
        P(),
        P("tp", None),
        P(),
        P(),
        P("ep", None),
        P("ep", None),
        P("ep", None, "tp"),
        P("ep", None, "tp"),
        P("ep", "tp", None),
        P(None, "tp"),
        P(None, "tp"),
        P("tp", None),
        P(),
        P(),
    )
    return jax.shard_map(
        local,
        mesh=mesh,
        in_specs=placed,
        out_specs=(P("ep", "tp"), P("ep", "tp", None, None)),
        check_vma=False,
    )
```

```python
import functools

import jax
import jax.numpy as jnp
from jax import lax
from jax.experimental import pallas as pl
from jax.experimental.pallas import tpu as pltpu
from jax.sharding import PartitionSpec as P

EPS = 1e-05
ALPHA = 2.0**0.25
MESH = pl.DeviceIdType.MESH
F32 = jnp.float32
BF16 = jnp.bfloat16
LANES = 128
HALF = 64

PH_HID, PH_MIX, PH_RS, PH_ROWS, PH_RET, PH_MOM, PH_SH, PH_EP, PH_PICK, PH_OUT = 0, 1, 2, 3, 4, 5, 6, 7, 10, 13
PH_HALF = 16
N_PH = 17
CLASSES = 3


def roll_half(x):
    return pltpu.roll(x, HALF, x.ndim - 1)


def low_lanes(shape):
    return lax.broadcasted_iota(jnp.int32, shape, len(shape) - 1) < HALF


def spread(k):
    return lax.div(k + 1, 2) * (2 * lax.rem(k, 2) - 1)


def spread_fixed(k):
    return ((k + 1) // 2) * (2 * (k % 2) - 1)


def wrap(i, n):
    return jnp.where(i >= n, i - n, i)


def finish(mixed_ref, state_ref, mixed_hbm, state_hbm, sems):
    copies = (
        pltpu.make_async_copy(state_ref, state_hbm, sems.at[0]),
        pltpu.make_async_copy(mixed_ref, mixed_hbm, sems.at[1]),
    )
    for copy in copies:
        copy.start()
    for copy in copies:
        copy.wait()


def kernel(n_tp, n_ep, n_x, *refs):
    hbm, refs = refs[:23], refs[23:]
    (out_ref, ns_ref), refs = refs[:2], refs[2:]
    vm, refs = refs[:23], refs[23:]
    (
        s16,
        s128,
        hid_t,
        hid_all,
        mix_s,
        mix_r,
        mix_low,
        mix_high,
        choose,
        rs_s,
        rs_r,
        row_t,
        row_all,
        ep_all,
        pick_t,
        pick_all,
        xrow,
        xnorm,
        sh_s,
        sh_r,
        out_s,
        out_r,
        line_s,
        line_r,
        half_s,
        half_r,
        ret_s,
        ret_r,
        mom_t,
        mom_all,
        lsem,
        ssem,
        rsem,
    ) = refs
    (
        hid_ref,
        routes_ref,
        rw_ref,
        wf,
        wi,
        wq,
        wg,
        lb_ref,
        hg_ref,
        state,
        wout,
        g1_ref,
        b1_ref,
        shg_ref,
        shu_ref,
        shd_ref,
        g1r_ref,
        b1r_ref,
        egu,
        ed,
        g2r_ref,
        b2r_ref,
    ) = vm[:22]
    egu_extra = hbm[22]

    g = lax.axis_index("ep")
    t = lax.axis_index("tp")
    core = lax.rem(g, 2)
    z = g // 2
    n_z = n_ep // 2
    n_y = n_tp // n_x
    y = t // n_x
    x = lax.rem(t, n_x)
    pairs = n_tp // 2
    seq = hid_ref.shape[0]
    width = n_tp * HALF
    per_class = n_ep // CLASSES
    rows_j = 2 * per_class

    barrier = pltpu.get_barrier_semaphore()

    chips = [wrap(z + (spread_fixed(k) + n_z) % n_z, n_z) for k in range(n_z)]

    def chip_behind(k):
        if 2 * spread_fixed(k) == n_z:
            return chips[k]
        return chips[k + 1 if k % 2 else k - 1]

    def ep_each(send):
        send(0, 2 * z + 1 - core)
        for k in range(1, n_z):
            for to_core in range(2):
                send(k, 2 * chip_behind(k) + to_core)

    def greet_tp(i, c):
        pl.semaphore_signal(barrier, inc=1, device_id={"tp": wrap(t + i, n_tp)}, device_id_type=MESH)
        return c

    pltpu.make_async_copy(hbm[0], hid_ref, lsem.at[0]).start()
    ep_each(
        lambda k, e: pl.semaphore_signal(barrier, inc=1, device_id={"ep": e}, device_id_type=MESH)
    )
    lax.fori_loop(1, n_tp, greet_tp, 0)

    columns = [wrap(x + dx, n_x) for dx in range(n_x)]
    by_distance = [n_x // 2] + [d for k in range(1, n_x) for d in [n_x // 2 + ((k + 1) // 2) * (2 * (k % 2) - 1)] if d % n_x] + [0]

    def tp_each(send):
        def body(k, c):
            base = n_x * wrap(y + n_y // 2 + spread(k), n_y)
            for dx in by_distance:
                send(base + columns[dx])
            return c

        lax.fori_loop(0, n_y - 1, body, 0)
        for dx in by_distance[:-1]:
            send(n_x * y + columns[dx])

    loads = []
    for i in range(22):
        if i == 18:
            loads.append(
                [
                    pltpu.make_async_copy(hbm[i], egu.at[:, :, 0:LANES], lsem.at[i]),
                    pltpu.make_async_copy(egu_extra, egu.at[:, :, LANES : 2 * LANES], lsem.at[22]),
                ]
            )
        else:
            loads.append([pltpu.make_async_copy(hbm[i], vm[i], lsem.at[i])])
    for group in loads[1:]:
        for load in group:
            load.start()

    def ready(*which):
        for i in which:
            for load in loads[i]:
                load.wait()

    def remote(src, dst, ph, device):
        return pltpu.make_async_remote_copy(
            src_ref=src,
            dst_ref=dst,
            send_sem=ssem.at[ph],
            recv_sem=rsem.at[ph],
            device_id=device,
            device_id_type=MESH,
        )

    def tp_tile(src, dst, ph):
        tp_each(lambda p: remote(src, dst.at[t], ph, {"tp": p}).start())

    def tp_tiles(src, dst, ph):
        tp_each(lambda p: remote(src.at[p], dst.at[t], ph, {"tp": p}).start())

    def whole(buf, count, ph):
        part = buf.at[pl.ds(0, count)]
        return remote(part, part, ph, {"tp": wrap(t + 1, n_tp)})

    low8 = low_lanes((8, LANES))
    s16[...] = jnp.zeros_like(s16)
    ready(0)
    s16[0:seq, 0:HALF] = hid_ref[...].astype(F32)
    hid_own = s16[0:8, :] + roll_half(s16[8:16, :])
    hid_t[...] = hid_own.astype(BF16)
    hid_all[t] = hid_own.astype(BF16)

    pl.semaphore_wait(barrier, n_ep + n_tp - 2)
    tp_tile(hid_t, hid_all, PH_HID)

    ready(1, 2)
    s128[...] = jnp.zeros_like(s128)
    s128[0:4, 0:seq] = routes_ref[...].astype(F32)
    s128[8:12, 0:seq] = rw_ref[...]
    by_row = jnp.transpose(s128[...])[0:16, :]
    lane16 = lax.broadcasted_iota(jnp.int32, (16, LANES), 1)
    row16 = lax.broadcasted_iota(jnp.int32, (16, LANES), 0)
    expert_of = (lane16 // 2).astype(F32)
    place_of = (lane16 % 2).astype(F32)
    named = jnp.zeros((16, LANES), F32)
    weight = jnp.zeros((16, LANES), F32)
    for k in range(4):
        hit = (by_row[:, k : k + 1] == expert_of) & (row16 < seq)
        named = named + jnp.where(hit, 1.0, 0.0)
        weight = weight + jnp.where(hit, by_row[:, 8 + k : 9 + k], 0.0)
    earlier = jnp.where(
        lax.broadcasted_iota(jnp.int32, (16, 16), 1) < lax.broadcasted_iota(jnp.int32, (16, 16), 0), 1.0, 0.0
    ).astype(BF16)
    before = jnp.dot(earlier, named.astype(BF16), preferred_element_type=F32)
    weight = jnp.where(before == place_of, weight, 0.0)
    s128[...] = jnp.zeros_like(s128)
    s128[0:16, :] = weight
    by_code = jnp.transpose(s128[...])
    lane32 = lax.broadcasted_iota(jnp.int32, (32, LANES), 1)
    row32 = lax.broadcasted_iota(jnp.int32, (32, LANES), 0)
    message = jnp.zeros((32, LANES), F32)
    for c in range(4):
        take = jnp.where(lane32 == 4 * row32 + c, 1.0, 0.0)
        part = jnp.dot(take, by_code, precision=lax.Precision.HIGHEST, preferred_element_type=F32)
        message = message + (part if c == 0 else pltpu.roll(part, 16 * c, 1))
    for e in range(n_ep):
        mix_s[e] = message[e : e + 1, :]
    mix_r[core] = mix_s[g]

    ep_each(lambda k, e: remote(mix_s.at[e], mix_r.at[2 * k + core], PH_MIX, {"ep": e}).start())

    def full_rows(buf):
        left, right = [], []
        for p in range(pairs):
            a = buf[2 * p].astype(F32)
            b = buf[2 * p + 1].astype(F32)
            left.append(jnp.where(low8, a, roll_half(b)))
            right.append(jnp.where(low8, roll_half(a), b))
        return jnp.concatenate([jnp.concatenate(left, 1), jnp.concatenate(right, 1)], 0)

    whole(hid_all, n_tp - 1, PH_HID).wait_recv()
    rows = full_rows(hid_all).astype(BF16)

    def project(i):
        ready(i)
        return jnp.dot(rows, vm[i][...], preferred_element_type=F32).astype(BF16).astype(F32)

    forget_pre = project(3)
    values = project(4)
    queries = project(5)
    queries = queries * jax.nn.sigmoid(queries)
    gate = project(6)
    gate = gate * jax.nn.sigmoid(gate)
    ready(7, 8)
    lower = lb_ref[...]
    forget = lower + (1.0 - lower) * jax.nn.sigmoid(forget_pre)
    key = (1.0 - lower) * jax.nn.sigmoid(-forget_pre)

    s128[0:16, :] = queries * forget
    by_channel = jnp.transpose(s128[...])
    ready(9)
    for b in range(seq):
        s16[b : b + 1, :] = jnp.sum(by_channel[:, b : b + 1] * state[b], axis=0, keepdims=True)
    s16[seq:16, :] = jnp.zeros((16 - seq, LANES), F32)
    readout = s16[...] + jnp.sum(queries * key, axis=1, keepdims=True) * values
    mean_sq = jnp.mean(readout * readout, axis=1, keepdims=True)
    mixed = (readout * lax.rsqrt(mean_sq + EPS) * hg_ref[...] * gate).astype(BF16)

    def fold_out(top, bottom, p, buf, at=lambda d: d):
        low = low_lanes(top.shape)
        buf[at(2 * p)] = jnp.where(low, top, roll_half(bottom)).astype(BF16)
        buf[at(2 * p + 1)] = jnp.where(low, roll_half(top), bottom).astype(BF16)

    def by_line(d):
        return d % n_x, d // n_x

    ready(10)
    branch = jnp.dot(mixed, wout[...], preferred_element_type=F32)
    for p in range(pairs):
        block = branch[:, p * LANES : (p + 1) * LANES]
        fold_out(block[0:8], block[8:16], p, rs_s)
    rs_r[t] = rs_s[t]
    tp_tiles(rs_s, rs_r, PH_RS)

    s128[0:16, :] = forget
    forget_col = jnp.transpose(s128[...])
    s128[0:16, :] = key
    key_col = jnp.transpose(s128[...])
    for b in range(seq):
        ns_ref[b] = forget_col[:, b : b + 1] * state[b] + key_col[:, b : b + 1] * values[b : b + 1, :]

    whole(mix_r, n_ep - 1, PH_MIX).wait_recv()
    lane8 = lax.broadcasted_iota(jnp.int32, (8, LANES), 1)
    row8 = lax.broadcasted_iota(jnp.int32, (8, LANES), 0)
    mask_low = (lane8 < HALF) & (lane8 % 16 == row8)
    mask_high = (lane8 < HALF) & (lane8 % 16 == row8 + 8)
    every = [jnp.broadcast_to(mix_r[r], (8, LANES)) for r in range(n_ep)]
    from_lane = lax.broadcasted_iota(jnp.int32, (LANES, LANES), 0)
    to_lane = lax.broadcasted_iota(jnp.int32, (LANES, LANES), 1)
    place = jnp.where(
        (from_lane < HALF) & (to_lane == (from_lane // 32) * rows_j + (from_lane // 16) % 2), 1.0, 0.0
    )
    for mask, keep in ((mask_low, mix_low), (mask_high, mix_high)):
        stacked = jnp.concatenate([jnp.where(mask, row, 0.0) for row in every], 0)
        placed = jnp.dot(stacked, place, precision=lax.Precision.HIGHEST, preferred_element_type=F32)
        for r in range(n_ep):
            at = 2 * (r % per_class)
            piece = placed[8 * r : 8 * r + 8]
            keep[r] = piece if at == 0 else pltpu.roll(piece, at, 1)
    for c in range(CLASSES):
        part = slice(c * per_class, (c + 1) * per_class)
        low_c = jnp.where(mix_low[part].reshape(8 * per_class, LANES) != 0.0, 1.0, 0.0)
        high_c = jnp.where(mix_high[part].reshape(8 * per_class, LANES) != 0.0, 1.0, 0.0)
        s128[0 : 8 * per_class, :] = low_c + pltpu.roll(high_c, 2 * rows_j, 1)
        choose[c] = jnp.transpose(s128[...])[0 : 4 * rows_j, 0 : 8 * per_class].astype(BF16)

    whole(rs_r, n_tp - 1, PH_RS).wait_recv()
    own = ALPHA * hid_own + jnp.sum(rs_r[...].astype(F32), axis=0)
    row_t[...] = own.astype(BF16)
    row_all[t] = own.astype(BF16)
    ep_all[core] = own.astype(BF16)

    ep_each(
        lambda k, e: remote(row_t, ep_all.at[2 * k + core], PH_EP + (2 * k) // per_class, {"ep": e}).start()
    )

    low_j = low_lanes((rows_j, LANES))
    one, two = slice(0, rows_j), slice(rows_j, 2 * rows_j)
    for c in range(CLASSES):
        whole(ep_all, per_class - 1 if c == 0 else per_class, PH_EP + c).wait_recv()
        tiles = ep_all[c * per_class : (c + 1) * per_class].astype(F32).reshape(8 * per_class, LANES).astype(BF16)
        got = jnp.dot(choose[c], tiles, preferred_element_type=F32)
        got_low, got_high = got[0 : 2 * rows_j], got[2 * rows_j : 4 * rows_j]
        picked = jnp.where(
            low_j,
            got_low[one] + roll_half(got_high[one]),
            roll_half(got_low[two]) + got_high[two],
        ).astype(BF16)
        pick_t[c] = picked
        pick_all[c, t] = picked
        tp_tile(pick_t.at[c], pick_all.at[c], PH_PICK + c)
        if c == 0:
            tp_tile(row_t, row_all, PH_ROWS)

    ready(11, 12, 13, 14, 15, 16, 17)
    whole(row_all, n_tp - 1, PH_ROWS).wait_recv()
    full = full_rows(row_all)
    mean1 = jnp.mean(full, axis=1, keepdims=True)
    centred = full - mean1
    rstd1 = lax.rsqrt(jnp.mean(centred * centred, axis=1, keepdims=True) + EPS)
    normed = (centred * rstd1 * g1_ref[...] + b1_ref[...]).astype(BF16)
    over_cols = (((1,), (1,)), ((), ()))
    sh_gate = lax.dot_general(normed, shg_ref[...], over_cols, preferred_element_type=F32)
    sh_up = lax.dot_general(normed, shu_ref[...], over_cols, preferred_element_type=F32)
    sh_hidden = (sh_gate * jax.nn.sigmoid(sh_gate) * sh_up).astype(BF16)
    shared = jnp.dot(sh_hidden, shd_ref[...], preferred_element_type=F32)
    for p in range(pairs):
        block = shared[:, p * LANES : (p + 1) * LANES]
        fold_out(block[0:8], block[8:16], p, sh_s)

    def own_columns(ref):
        row = jnp.broadcast_to(ref[pl.ds(t // 2, 1), :], (8, LANES))
        swapped = roll_half(row)
        even = lax.rem(t, 2) == 0
        return jnp.where(low8, jnp.where(even, row, swapped), jnp.where(even, swapped, row))

    def fold_rows(col):
        return jnp.where(low8, col[0:8], col[8:16])

    own_normed = ((own - fold_rows(mean1)) * fold_rows(rstd1) * own_columns(g1r_ref) + own_columns(b1r_ref)).astype(
        BF16
    ).astype(F32)

    ready(18, 19)
    for c in range(CLASSES):
        whole(pick_all.at[c], n_tp - 1, PH_PICK + c).wait_recv()
        sums = [jnp.zeros((rows_j, LANES), F32), jnp.zeros((rows_j, LANES), F32)]
        for p in range(pairs):
            a = pick_all[c, 2 * p].astype(F32)
            b = pick_all[c, 2 * p + 1].astype(F32)
            cols = slice(p * LANES, (p + 1) * LANES)
            x0 = jnp.where(low_j, a, roll_half(b))
            x1 = jnp.where(low_j, roll_half(a), b)
            xrow[one, cols] = x0
            xrow[two, cols] = x1
            sums = [sums[0] + x0, sums[1] + x1]
        hidden = []
        for j, at in enumerate((one, two)):
            mean = jnp.sum(sums[j], axis=1, keepdims=True) / width
            total = jnp.zeros((rows_j, LANES), F32)
            for p in range(pairs):
                d = xrow[at, p * LANES : (p + 1) * LANES] - mean
                total = total + d * d
            rstd = lax.rsqrt(jnp.sum(total, axis=1, keepdims=True) / width + EPS)
            for p in range(pairs):
                cols = slice(p * LANES, (p + 1) * LANES)
                xnorm[at, cols] = ((xrow[at, cols] - mean) * rstd * g1_ref[:, cols] + b1_ref[:, cols]).astype(BF16)
            both = jnp.dot(xnorm[at, :], egu[j], preferred_element_type=F32)
            gate_j, up_j = both[:, 0:LANES], both[:, LANES : 2 * LANES]
            hidden.append((gate_j * jax.nn.sigmoid(gate_j) * up_j).astype(BF16))
        step = min(256, width)
        for n in range(width // step):
            cols = slice(n * step, (n + 1) * step)
            y0 = jnp.dot(hidden[0], ed[0, :, cols], preferred_element_type=F32)
            y1 = jnp.dot(hidden[1], ed[1, :, cols], preferred_element_type=F32)
            for q in range(step // LANES):
                sub = slice(q * LANES, (q + 1) * LANES)
                p = n * (step // LANES) + q
                if c == 0:
                    fold_out(y0[:, sub], y1[:, sub], p, line_s, by_line)
                else:
                    fold_out(y0[:, sub], y1[:, sub], p, out_s.at[c - 1])
        if c == 0:
            line_r[x] = line_s[x]
            for d in by_distance[:-1]:
                remote(line_s.at[columns[d]], line_r.at[x], PH_HALF, {"tp": n_x * y + columns[d]}).start()
        else:
            out_r[c - 1, t] = out_s[c - 1, t]
            tp_tiles(out_s.at[c - 1], out_r.at[c - 1], PH_OUT + c)
        if c == 1:
            whole(line_r, n_x - 1, PH_HALF).wait_recv()
            half_s[...] = jnp.sum(line_r[...].astype(F32), axis=0).astype(BF16)
            half_r[y] = half_s[y]

            def half_send(d, carry):
                to_y = wrap(y + d, n_y)
                remote(half_s.at[to_y], half_r.at[y], PH_OUT, {"tp": n_x * to_y + x}).start()
                return carry

            lax.fori_loop(1, n_y, half_send, 0)
        if c == CLASSES - 1:
            sh_r[t] = sh_s[t]
            tp_tiles(sh_s, sh_r, PH_SH)

    for c in range(CLASSES):
        if c == 0:
            whole(half_r, n_y - 1, PH_OUT).wait_recv()
            slots = jnp.sum(half_r[...].astype(F32), axis=0)
        else:
            whole(out_r.at[c - 1], n_tp - 1, PH_OUT + c).wait_recv()
            slots = jnp.sum(out_r[c - 1].astype(F32), axis=0)
        turned = roll_half(slots)
        both = jnp.concatenate([jnp.where(low_j, slots, turned), jnp.where(low_j, turned, slots)], 0)
        part = slice(c * per_class, (c + 1) * per_class)
        low_c = mix_low[part].reshape(8 * per_class, LANES)[:, 0 : 2 * rows_j]
        high_c = mix_high[part].reshape(8 * per_class, LANES)[:, 0 : 2 * rows_j]
        back_low = jnp.dot(low_c, both, precision=lax.Precision.HIGHEST, preferred_element_type=F32)
        back_high = jnp.dot(high_c, both, precision=lax.Precision.HIGHEST, preferred_element_type=F32)
        back = jnp.where(low_lanes((8 * per_class, LANES)), back_low, back_high)
        ret_s[part] = back.reshape(per_class, 8, LANES).astype(BF16)
        if c == 0:
            ret_r[g] = ret_s[core]

        def ret_send(r, e):
            remote(ret_s.at[r], ret_r.at[g], PH_RET, {"ep": e}).start()

        for k in range(c * per_class // 2, (c + 1) * per_class // 2):
            if k == 0:
                ret_send(1 - core, 2 * z + 1 - core)
            else:
                for from_core in range(2):
                    ret_send(2 * k + from_core, 2 * chips[k] + from_core)

    ready(20, 21)
    whole(sh_r, n_tp - 1, PH_SH).wait_recv()
    final = ALPHA * own_normed + jnp.sum(sh_r[...].astype(F32), axis=0)
    whole(ret_r, n_ep - 1, PH_RET).wait_recv()
    final = final + jnp.sum(ret_r[...].astype(F32), axis=0)

    mine = jnp.concatenate([jnp.where(low8, final, 0.0), jnp.where(low8, roll_half(final), 0.0)], 0)
    part = jnp.where(lane16 == row16, jnp.sum(mine, axis=1, keepdims=True), 0.0) + jnp.where(
        lane16 == row16 + 16, jnp.sum(mine * mine, axis=1, keepdims=True), 0.0
    )
    part = jnp.sum(part, axis=0, keepdims=True)
    mom_t[...] = part
    mom_all[t] = part
    tp_tile(mom_t, mom_all, PH_MOM)
    for buf, count, ph in (
        (hid_all, n_tp - 1, PH_HID),
        (mix_r, n_ep - 1, PH_MIX),
        (rs_r, n_tp - 1, PH_RS),
        (row_all, n_tp - 1, PH_ROWS),
        (sh_r, n_tp - 1, PH_SH),
        (ret_r, n_ep - 1, PH_RET),
    ):
        whole(buf, count, ph).wait_send()
    for c in range(CLASSES):
        whole(ep_all, per_class - 1 if c == 0 else per_class, PH_EP + c).wait_send()
        whole(pick_all.at[c], n_tp - 1, PH_PICK + c).wait_send()
        if c == 0:
            whole(line_r, n_x - 1, PH_HALF).wait_send()
            whole(half_r, n_y - 1, PH_OUT).wait_send()
        else:
            whole(out_r.at[c - 1], n_tp - 1, PH_OUT + c).wait_send()
    whole(mom_all, n_tp - 1, PH_MOM).wait_recv()
    moments = jnp.broadcast_to(jnp.sum(mom_all[...], axis=0) / width, (16, LANES))
    mean2 = jnp.sum(jnp.where(lane16 == row16, moments, 0.0), axis=1, keepdims=True)
    square2 = jnp.sum(jnp.where(lane16 == row16 + 16, moments, 0.0), axis=1, keepdims=True)
    rstd2 = lax.rsqrt(square2 - mean2 * mean2 + EPS)
    done = (final - fold_rows(mean2)) * fold_rows(rstd2) * own_columns(g2r_ref) + own_columns(b2r_ref)
    s16[0:8, :] = done
    s16[8:16, :] = roll_half(done)
    out_ref[...] = s16[0:seq, 0:HALF].astype(BF16)
    whole(mom_all, n_tp - 1, PH_MOM).wait_send()


def local(
    hidden_in,
    state,
    lower_bound,
    w_forget,
    w_input,
    w_query,
    w_outgate,
    head_gain,
    w_out,
    ln1_gain,
    ln1_bias,
    routes,
    route_weights,
    exp_gate,
    exp_up,
    exp_down,
    sh_gate,
    sh_up,
    sh_down,
    ln2_gain,
    ln2_bias,
):
    n_tp = lax.axis_size("tp")
    n_ep = lax.axis_size("ep")
    n_x = 4
    seq = hidden_in.shape[0]
    width = w_forget.shape[0]
    per_class = n_ep // CLASSES
    rows_j = 2 * per_class
    operands = (
        hidden_in,
        routes.T,
        route_weights.T,
        w_forget,
        w_input,
        w_query,
        w_outgate,
        lower_bound,
        head_gain.reshape(1, LANES),
        state.reshape(seq, LANES, LANES),
        w_out,
        ln1_gain.reshape(1, width),
        ln1_bias.reshape(1, width),
        sh_gate.T,
        sh_up.T,
        sh_down,
        ln1_gain.reshape(width // LANES, LANES),
        ln1_bias.reshape(width // LANES, LANES),
        exp_gate,
        exp_down,
        ln2_gain.reshape(width // LANES, LANES),
        ln2_bias.reshape(width // LANES, LANES),
        exp_up,
    )
    held = [pltpu.VMEM(a.shape, a.dtype) for a in operands]
    held[18] = pltpu.VMEM((2, width, 2 * LANES), BF16)
    held[22] = pltpu.VMEM((8, LANES), F32)
    vmem = pl.BlockSpec(memory_space=pltpu.VMEM)
    hbm = pl.BlockSpec(memory_space=pltpu.HBM)
    sem = pltpu.SemaphoreType.DMA
    tile = (8, LANES)
    mixed_out, new_state = pl.pallas_call(
        functools.partial(kernel, n_tp, n_ep, n_x),
        out_shape=(pltpu.VMEM(hidden_in.shape, BF16), pltpu.VMEM((seq, LANES, LANES), F32)),
        in_specs=[hbm] * len(operands),
        out_specs=(vmem, vmem),
        scratch_shapes=[
            *held,
            pltpu.VMEM((16, LANES), F32),
            pltpu.VMEM((LANES, LANES), F32),
            pltpu.VMEM(tile, BF16),
            pltpu.VMEM((n_tp, *tile), BF16),
            pltpu.VMEM((n_ep, 1, LANES), F32),
            pltpu.VMEM((n_ep, 1, LANES), F32),
            pltpu.VMEM((n_ep, *tile), F32),
            pltpu.VMEM((n_ep, *tile), F32),
            pltpu.VMEM((CLASSES, 4 * rows_j, 8 * per_class), BF16),
            pltpu.VMEM((n_tp, *tile), BF16),
            pltpu.VMEM((n_tp, *tile), BF16),
            pltpu.VMEM(tile, BF16),
            pltpu.VMEM((n_tp, *tile), BF16),
            pltpu.VMEM((n_ep, *tile), BF16),
            pltpu.VMEM((CLASSES, rows_j, LANES), BF16),
            pltpu.VMEM((CLASSES, n_tp, rows_j, LANES), BF16),
            pltpu.VMEM((2 * rows_j, width), F32),
            pltpu.VMEM((2 * rows_j, width), BF16),
            pltpu.VMEM((n_tp, *tile), BF16),
            pltpu.VMEM((n_tp, *tile), BF16),
            pltpu.VMEM((CLASSES - 1, n_tp, rows_j, LANES), BF16),
            pltpu.VMEM((CLASSES - 1, n_tp, rows_j, LANES), BF16),
            pltpu.VMEM((n_x, n_tp // n_x, rows_j, LANES), BF16),
            pltpu.VMEM((n_x, n_tp // n_x, rows_j, LANES), BF16),
            pltpu.VMEM((n_tp // n_x, rows_j, LANES), BF16),
            pltpu.VMEM((n_tp // n_x, rows_j, LANES), BF16),
            pltpu.VMEM((n_ep, *tile), BF16),
            pltpu.VMEM((n_ep, *tile), BF16),
            pltpu.VMEM((1, LANES), F32),
            pltpu.VMEM((n_tp, 1, LANES), F32),
            sem((24,)),
            sem((N_PH,)),
            sem((N_PH,)),
        ],
        compiler_params=pltpu.CompilerParams(collective_id=0, has_side_effects=True),
        name="decode_step",
    )(*operands)
    mixed_out, new_state = pl.pallas_call(
        finish,
        out_shape=(
            jax.ShapeDtypeStruct(hidden_in.shape, BF16),
            jax.ShapeDtypeStruct((seq, LANES, LANES), F32),
        ),
        in_specs=[vmem] * 2,
        out_specs=(hbm, hbm),
        scratch_shapes=[sem((2,))],
        name="write_out",
    )(
        pltpu.with_memory_space_constraint(mixed_out, pltpu.VMEM),
        pltpu.with_memory_space_constraint(new_state, pltpu.VMEM),
    )
    return (mixed_out, new_state.reshape(state.shape))


def solution(mesh):
    placed = (
        P("ep", "tp"),
        P("ep", "tp", None, None),
        P("tp", None),
        P(None, "tp"),
        P(None, "tp"),
        P(None, "tp"),
        P(None, "tp"),
        P(),
        P("tp", None),
        P(),
        P(),
        P("ep", None),
        P("ep", None),
        P("ep", None, "tp"),
        P("ep", None, "tp"),
        P("ep", "tp", None),
        P(None, "tp"),
        P(None, "tp"),
        P("tp", None),
        P(),
        P(),
    )
    return jax.shard_map(
        local,
        mesh=mesh,
        in_specs=placed,
        out_specs=(P("ep", "tp"), P("ep", "tp", None, None)),
        check_vma=False,
    )
```
